256 devices in a mesh: sp: 64 (over z, x, core), tp: 4 (over y).
Axes of the slice: x: 4, y: 4, z: 8, core: 2. Of those that a mesh axis runs over, the one named last changes fastest.
Arguments:
- query_nope: bfloat16 [16384, 1024], P('sp', 'tp'), may hold values from -24 to 24
- query_rope: bfloat16 [16384, 512], P('sp', 'tp'), may hold values from -384 to 384
- latent: bfloat16 [16384, 256], P('sp'), may hold values from -6 to 6
- key_rope: bfloat16 [16384, 64], P('sp'), may hold values from -8 to 8
- latent_gain: bfloat16 [256], replicated, may hold values from 0.099609375 to 1.8984375
- key_up: bfloat16 [256, 1024], replicated, may hold values from -0.375 to 0.375
- value_up: bfloat16 [256, 1024], replicated, may hold values from -0.375 to 0.375
- out_proj: bfloat16 [1024, 2048], P('tp'), may hold values from -0.1875 to 0.1875
- residual: bfloat16 [16384, 2048], P(('sp', 'tp')), may hold values from -6 to 6
- ffn_gain: bfloat16 [2048], replicated, may hold values from 0.099609375 to 1.8984375
- expert_ids: int32 [16384, 4], P(('sp', 'tp')), may hold values from 0 to 63, all different within a row; in each aligned block of 64 rows (0 to 63, 64 to 127, ...) at most 8 rows name the same one
- route_weights: float32 [16384, 4], P(('sp', 'tp')), may hold values from 0.1 to 1
- expert_gate: bfloat16 [64, 2048, 384], P('sp'), may hold values from -0.125 to 0.125
- expert_up: bfloat16 [64, 2048, 384], P('sp'), may hold values from -0.125 to 0.125
- expert_down: bfloat16 [64, 384, 2048], P('sp'), may hold values from -0.3125 to 0.3125
- shared_gate: bfloat16 [2048, 384], replicated, may hold values from -0.125 to 0.125
- shared_up: bfloat16 [2048, 384], replicated, may hold values from -0.125 to 0.125
- shared_down: bfloat16 [384, 2048], replicated, may hold values from -0.3125 to 0.3125
Outputs:
- layer_out: bfloat16 [16384, 2048], P(('sp', 'tp'))
The draws below stay inside these ranges and needn't reach their ends.
Inputs may be any that keep to these rules, and one draw needn't show every extreme that they name: `expert_ids`: each row names 4 different experts; among the 64 rows of one aligned block no expert is named by more than 8 rows.
All inputs are finite; a program needn't handle non-finite values.
Results may differ from the reference program's by a relative error of at most 0.017.
Values may be sent and summed in bfloat16 or wider, within the bound.
A program may use at most 128 MiB of HBM per device.

```python
import math
import jax
import jax.numpy as jnp
import numpy as np
from jax import lax

D = 2048
HEADS = 8
NOPE = 128
ROPE = 64
VDIM = 128
KV_RANK = 256
FF = 384
TOP = 4
EXPERTS = 64
SEQ = 16384
TOK_DEV = 64
CAP = 8
N_TP = 4


def draw_query_nope(key, part):
    own_key = jax.random.fold_in(key, 1)
    base_draw = 4.0 * jax.random.truncated_normal(own_key, -6.0, 6.0, (SEQ, HEADS * NOPE), jnp.float32)
    return base_draw.astype(jnp.bfloat16)


def draw_query_rope(key, part):
    own_key = jax.random.fold_in(key, 2)
    base_draw = 4.0 * jax.random.truncated_normal(own_key, -6.0, 6.0, (SEQ, HEADS * ROPE), jnp.float32)
    return base_draw.astype(jnp.bfloat16)


def draw_key_rope(key, part):
    own_key = jax.random.fold_in(key, 3)
    base_draw = jax.random.truncated_normal(own_key, -6.0, 6.0, (SEQ, ROPE), jnp.float32)
    return base_draw.astype(jnp.bfloat16)


def shard_levels(stream_key, dims, cuts, smallest, high):
    def one(dim, blocks):
        heights = jax.random.uniform(jax.random.fold_in(jax.random.fold_in(stream_key, 6), dim), (blocks,), jnp.float32, smallest / len(cuts), high / len(cuts))
        return jnp.repeat(jnp.exp(heights), dims[dim] // blocks).reshape((-1,) + (1,) * (len(dims) - dim - 1))

    level = one(*cuts[0])
    for cut in cuts[1:]:
        level = level * one(*cut)
    return level


def shared_out(key, own, number, rows, count, top, limit, skew):
    order = jax.random.permutation(key, count)
    crowded, ordinary = portions_of(count, rows * top, limit, skew, True), portions_of(count, rows * top, limit, skew, False)
    places = jnp.arange(count)

    def named(tallies, rotation):
        used = int((tallies > 0).sum())
        fixed = max(1, used // 4)
        moved = fixed + (places - fixed + rotation * (used - fixed)) % max(1, count - fixed)
        return jnp.zeros((count,), jnp.int32).at[order[jnp.where(places < fixed, places, moved)]].set(jnp.asarray(tallies, jnp.int32))

    tallies = jnp.where(number % 4 == 0, named(crowded, number // 4), named(ordinary, number - number // 4 - 1))
    mixed = jax.random.permutation(jax.random.fold_in(own, 3), count)
    donor, sink = mixed[0:count // 2 * 2:2], mixed[1:count // 2 * 2:2]
    slack = jnp.minimum(tallies[donor] - 1, limit - tallies[sink]) // 2
    slack = jnp.where((donor == order[0]) | (sink == order[0]) | (tallies[sink] == 0), 0, jnp.maximum(slack, 0))
    moved = jax.random.randint(jax.random.fold_in(own, 4), (count // 2,), 0, 1 << 20) % (slack + 1)
    tallies = tallies.at[donor].add(-moved).at[sink].add(moved)
    labels = jnp.searchsorted(jnp.cumsum(tallies), jnp.arange(rows * top), side="right").astype(jnp.int32)
    grid = labels.reshape(top, rows).T
    grid = grid[jax.random.permutation(jax.random.fold_in(own, 1), rows)]
    rotation = jax.random.randint(jax.random.fold_in(own, 2), (rows, 1), 0, top)
    return jnp.take_along_axis(grid, (jnp.arange(top)[None, :] + rotation) % top, axis=1)


def portions_of(number_of, total, limit, lean, full):
    loads = [(1 << 20) // math.isqrt(standing ** lean) + 1 for standing in range(1, number_of + 1)]
    largest = limit if full else min(limit, max(-(-total // number_of), total * loads[0] // sum(loads)))
    least = 1 if total - largest >= number_of - 1 else 0
    holding, spare = [largest] + [least] * (number_of - 1), total - largest - least * (number_of - 1)
    while spare > 0:
        movable = [i for i in range(1, number_of) if holding[i] < largest] or [i for i in range(1, number_of) if holding[i] < limit]
        mass, remaining = sum([loads[i] for i in movable]), spare
        for i in movable:
            more = min(limit - holding[i], max(1, remaining * loads[i] // mass), spare)
            holding[i] = holding[i] + more
            spare = spare - more
    return np.array(holding)


def scatter_about(key, shape, width, bound, shards=(), kind=jnp.bfloat16):
    factor_of = shard_levels(key, shape, shards, -0.22, 0.18) if shards else 1.0
    values = jax.random.normal(key, shape, jnp.float32) * width * factor_of
    return jnp.minimum(jnp.maximum(values, -bound), bound).astype(kind)


def setup_inputs(seed: int = 0) -> dict:
    keys = jax.random.split(jax.random.key(seed), 19)
    query_nope = draw_query_nope(jax.random.fold_in(keys[18], 71), 0)
    query_rope = draw_query_rope(jax.random.fold_in(keys[18], 71), 0)
    latent = scatter_about(keys[2], (SEQ, KV_RANK), 1.0, 6.0, ((0, 64),))
    key_rope = draw_key_rope(jax.random.fold_in(keys[18], 71), 0)
    latent_gain = jnp.clip(1.0 + 0.18 * jax.random.normal(keys[4], (KV_RANK,), jnp.float32), 0.099609375, 1.8984375).astype(jnp.bfloat16)
    key_up = scatter_about(keys[5], (KV_RANK, HEADS * NOPE), KV_RANK ** -0.5, 0.375)
    value_up = scatter_about(keys[6], (KV_RANK, HEADS * VDIM), KV_RANK ** -0.5, 0.375)
    out_proj = scatter_about(keys[7], (HEADS * VDIM, D), (HEADS * VDIM) ** -0.5, 0.1875, ((0, 4),))
    residual = scatter_about(keys[8], (SEQ, D), 1.0, 6.0, ((0, 256),))
    ffn_gain = jnp.clip(1.0 + 0.18 * jax.random.normal(keys[9], (D,), jnp.float32), 0.099609375, 1.8984375).astype(jnp.bfloat16)
    expert_ids_keys = jax.random.split(jax.random.fold_in(keys[10], 1), SEQ // TOK_DEV)
    expert_ids_turns = jax.random.permutation(jax.random.fold_in(keys[10], 3), SEQ // TOK_DEV)
    expert_ids = jax.vmap(lambda own, number: shared_out(jax.random.fold_in(keys[10], 2), own, number, TOK_DEV, EXPERTS, TOP, CAP, 1))(expert_ids_keys, expert_ids_turns).reshape((SEQ, TOP))
    route_weights = jnp.clip(jnp.exp(math.log(1.0) - 2.3025851 * jax.random.uniform(keys[11], (SEQ, TOP), jnp.float32) ** shard_levels(keys[11], (SEQ, TOP), ((0, 256),), -0.2, 0.2)), 0.1, 1.0)
    expert_gate = scatter_about(keys[12], (EXPERTS, D, FF), D ** -0.5, 0.125, ((0, 64),))
    expert_up = scatter_about(keys[13], (EXPERTS, D, FF), D ** -0.5, 0.125, ((0, 64),))
    expert_down = scatter_about(keys[14], (EXPERTS, FF, D), FF ** -0.5, 0.3125, ((0, 64),))
    shared_gate = scatter_about(keys[15], (D, FF), D ** -0.5, 0.125)
    shared_up = scatter_about(keys[16], (D, FF), D ** -0.5, 0.125)
    shared_down = scatter_about(keys[17], (FF, D), FF ** -0.5, 0.3125)
    return {"query_nope": query_nope, "query_rope": query_rope, "latent": latent, "key_rope": key_rope, "latent_gain": latent_gain, "key_up": key_up, "value_up": value_up, "out_proj": out_proj, "residual": residual, "ffn_gain": ffn_gain, "expert_ids": expert_ids, "route_weights": route_weights, "expert_gate": expert_gate, "expert_up": expert_up, "expert_down": expert_down, "shared_gate": shared_gate, "shared_up": shared_up, "shared_down": shared_down}


rope_base = 10000.0
norm_eps = 1e-06

def scale_rows(values, gain_vec):
    as_float = values.astype(jnp.float32)
    factor = lax.rsqrt(lax.optimization_barrier(jnp.mean(as_float * as_float, axis=-1, keepdims=True)) + norm_eps)
    return (as_float * factor * gain_vec.astype(jnp.float32)).astype(jnp.bfloat16)

def rotate(values, positions):
    half_dim = values.shape[-1] // 2
    frequency = rope_base ** (-jnp.arange(half_dim, dtype=jnp.float32) / half_dim)
    angles = positions.astype(jnp.float32)[:, None, None] * frequency
    cosine = jnp.cos(angles)
    sine_part = jnp.sin(angles)
    as_float = values.astype(jnp.float32)
    first_half = as_float[..., :half_dim]
    second_half = as_float[..., half_dim:]
    return jnp.concatenate([first_half * cosine - second_half * sine_part, first_half * sine_part + second_half * cosine], axis=-1).astype(jnp.bfloat16)

def reference(query_nope, query_rope, latent, key_rope, latent_gain, key_up, value_up, out_proj, residual, ffn_gain, expert_ids, route_weights, expert_gate, expert_up, expert_down, shared_gate, shared_up, shared_down):
    length = latent.shape[0]
    model_width = residual.shape[1]
    positions = jnp.arange(length, dtype=jnp.int32)
    normed_latent = scale_rows(latent, latent_gain)
    keys_nope = jnp.dot(normed_latent, key_up, preferred_element_type=jnp.float32).astype(jnp.bfloat16)
    values = jnp.dot(normed_latent, value_up, preferred_element_type=jnp.float32).astype(jnp.bfloat16)
    key_heads = keys_nope.reshape(length, HEADS, NOPE).astype(jnp.float32)
    value_heads = values.reshape(length, HEADS, VDIM).astype(jnp.float32)
    rot_key = rotate(key_rope[:, None, :], positions)[:, 0, :].astype(jnp.float32)
    queries_nope = query_nope.reshape(length, HEADS, NOPE)
    rot_query = rotate(query_rope.reshape(length, HEADS, ROPE), positions)
    block_len = math.gcd(length, 512)
    score_scale = 1.0 / math.sqrt(NOPE + ROPE)

    def one_block(block_start):
        query_part = lax.dynamic_slice_in_dim(queries_nope, block_start, block_len, 0).astype(jnp.float32)
        rotary_part = lax.dynamic_slice_in_dim(rot_query, block_start, block_len, 0).astype(jnp.float32)
        scores = jnp.einsum('qhd,khd->hqk', query_part, key_heads)
        scores = (scores + jnp.einsum('qhd,kd->hqk', rotary_part, rot_key)) * score_scale
        query_pos = block_start + jnp.arange(block_len, dtype=jnp.int32)
        allowed = (positions[None, :] <= query_pos[:, None])[None]
        scores = jnp.where(allowed, scores, -1e+30)
        highest = lax.optimization_barrier(jnp.max(scores, axis=-1, keepdims=True))
        weights = jnp.where(allowed, jnp.exp(scores - highest), 0.0)
        denominators = lax.optimization_barrier(jnp.sum(weights, axis=-1))
        rounded_weights = lax.optimization_barrier(weights.astype(jnp.bfloat16))
        mixed = jnp.einsum('hqk,khd->qhd', rounded_weights.astype(jnp.float32), value_heads)
        return (mixed / denominators.T[:, :, None]).astype(jnp.bfloat16)
    starts = jnp.arange(length // block_len, dtype=jnp.int32) * block_len
    heads_out = lax.map(one_block, starts).reshape(length, HEADS * VDIM)
    group_width = HEADS * VDIM // N_TP
    attn_sum = jnp.zeros((length, model_width), jnp.float32)
    for group_index in range(N_TP):
        partial_rows = jnp.dot(heads_out[:, group_index * group_width:(group_index + 1) * group_width], out_proj[group_index * group_width:(group_index + 1) * group_width], preferred_element_type=jnp.float32)
        rounded_rows = lax.optimization_barrier(partial_rows.astype(jnp.bfloat16))
        attn_sum = attn_sum + rounded_rows.astype(jnp.float32)
    hidden_one = (residual.astype(jnp.float32) + attn_sum).astype(jnp.bfloat16)
    normed = scale_rows(hidden_one, ffn_gain)
    row_total = length * TOP
    flat_ids = expert_ids.reshape(-1).astype(jnp.int32)
    onehot = (flat_ids[:, None] == jnp.arange(EXPERTS, dtype=jnp.int32)[None, :]).astype(jnp.int32)
    slot_rank = lax.optimization_barrier(jnp.sum(jnp.cumsum(onehot, axis=0) * onehot, axis=1)) - 1
    most_rows = length // TOK_DEV * CAP
    target = (flat_ids * most_rows + slot_rank).astype(jnp.int32)
    slot_token = jnp.full((EXPERTS * most_rows,), length, jnp.int32).at[target].set(jnp.arange(row_total, dtype=jnp.int32) // TOP)
    slot_weight = jnp.zeros((EXPERTS * most_rows,), jnp.float32).at[target].set(route_weights.reshape(-1).astype(jnp.float32))
    padded = jnp.concatenate([normed, jnp.zeros((1, model_width), jnp.bfloat16)], axis=0)

    def one_expert(accum, expert_index):
        picks = lax.dynamic_slice_in_dim(slot_token, expert_index * most_rows, most_rows, 0)
        chosen = padded[picks]
        gate_part = jnp.dot(chosen, expert_gate[expert_index], preferred_element_type=jnp.float32)
        upper_part = jnp.dot(chosen, expert_up[expert_index], preferred_element_type=jnp.float32)
        expert_hidden = (jax.nn.silu(gate_part) * upper_part).astype(jnp.bfloat16)
        expert_rows = jnp.dot(expert_hidden, expert_down[expert_index], preferred_element_type=jnp.float32).astype(jnp.bfloat16)
        scaled = expert_rows.astype(jnp.float32) * lax.dynamic_slice_in_dim(slot_weight, expert_index * most_rows, most_rows, 0)[:, None]
        return (accum.at[picks].add(scaled), expert_index)
    accum = lax.scan(one_expert, jnp.zeros((length + 1, model_width), jnp.float32), jnp.arange(EXPERTS, dtype=jnp.int32))[0]
    routed = accum[:length].astype(jnp.bfloat16)
    shared_gate_part = jnp.dot(normed, shared_gate, preferred_element_type=jnp.float32)
    shared_upper = jnp.dot(normed, shared_up, preferred_element_type=jnp.float32)
    shared_hidden = (jax.nn.silu(shared_gate_part) * shared_upper).astype(jnp.bfloat16)
    shared_rows = jnp.dot(shared_hidden, shared_down, preferred_element_type=jnp.float32).astype(jnp.bfloat16)
    return (hidden_one.astype(jnp.float32) + routed.astype(jnp.float32) + shared_rows.astype(jnp.float32)).astype(jnp.bfloat16)
```

```python
import math

import jax
import jax.numpy as jnp
from jax import lax
from jax.experimental import pallas as pl
from jax.experimental.pallas import tpu as pltpu
from jax.sharding import Mesh, PartitionSpec as P

NOPE = 128
ROPE = 64
VDIM = 128
NZ, NX, NC, NY = 8, 4, 2, 4
CAP = 8
ROWS = 256
QUART = 64
PACK = 80

rope_base = 10000.0
norm_eps = 1e-06


def scale_rows(values, gain_vec):
    as_float = values.astype(jnp.float32)
    factor = lax.rsqrt(jnp.mean(as_float * as_float, axis=-1, keepdims=True) + norm_eps)
    return (as_float * factor * gain_vec.astype(jnp.float32)).astype(jnp.bfloat16)


def rotate(values, positions):
    half_dim = values.shape[-1] // 2
    frequency = rope_base ** (-jnp.arange(half_dim, dtype=jnp.float32) / half_dim)
    angles = positions.astype(jnp.float32)[:, None, None] * frequency
    cosine = jnp.cos(angles)
    sine_part = jnp.sin(angles)
    as_float = values.astype(jnp.float32)
    first_half = as_float[..., :half_dim]
    second_half = as_float[..., half_dim:]
    return jnp.concatenate(
        [
            first_half * cosine - second_half * sine_part,
            first_half * sine_part + second_half * cosine,
        ],
        axis=-1,
    ).astype(jnp.bfloat16)


KB = 4
LOG2E = 1.4426950408889634


def attend_kernel(first, last, meta, q_ref, g_ref, ku_ref, vu_ref, *refs):
    if first:
        state_in = None
        outs = refs[:1] if last else refs[:3]
        m_ref, l_ref, acc_ref = refs[-3:]
    else:
        mi_ref, li_ref, ai_ref = refs[:3]
        outs = refs[3:4] if last else refs[3:6]
        m_ref, l_ref, acc_ref = refs[-3:]
    i = pl.program_id(0)
    nsteps = pl.num_programs(0)
    q_sp = meta[0]
    core = meta[1]
    needed = meta[2]
    whole = meta[3]
    scale = LOG2E / math.sqrt(NOPE + ROPE)

    @pl.when(i == 0)
    def _():
        if first:
            m_ref[...] = jnp.full(m_ref.shape, -1e30, jnp.float32)
            l_ref[...] = jnp.zeros(l_ref.shape, jnp.float32)
            acc_ref[...] = jnp.zeros(acc_ref.shape, jnp.float32)
        else:
            m_ref[...] = mi_ref[...]
            l_ref[...] = li_ref[...]
            acc_ref[...] = ai_ref[...]

    def step(masked):
        keys = KB * ROWS
        lat = jnp.concatenate(
            [g_ref[b, y, 0:QUART, :] for b in range(KB) for y in range(NY)], axis=0
        )
        rope = jnp.concatenate(
            [
                g_ref[b, y, QUART:PACK, g * ROPE : (g + 1) * ROPE]
                for b in range(KB)
                for y in range(NY)
                for g in range(4)
            ],
            axis=0,
        )
        rope = jnp.concatenate([rope, jnp.zeros((keys, ROPE), jnp.bfloat16)], axis=1)
        k = jnp.dot(lat, ku_ref[...], preferred_element_type=jnp.float32).astype(jnp.bfloat16)
        v = jnp.dot(lat, vu_ref[...], preferred_element_type=jnp.float32).astype(jnp.bfloat16)
        if masked:
            j = lax.broadcasted_iota(jnp.int32, (1, keys), 1)
            chunk = i * KB + j // ROWS
            kpos = (chunk * 2 + core) * ROWS + j % ROWS
            qpos = q_sp * ROWS + lax.broadcasted_iota(jnp.int32, (ROWS, 1), 0)
            allowed = kpos <= qpos
        for h in range(2):
            kcat = jnp.concatenate([k[:, h * NOPE : (h + 1) * NOPE], rope], axis=1)
            s = lax.dot_general(
                q_ref[h], kcat, (((1,), (1,)), ((), ())), preferred_element_type=jnp.float32
            )
            s = s * scale
            if masked:
                s = jnp.where(allowed, s, -1e30)
            m_old = m_ref[h]
            m_new = jnp.maximum(m_old, jnp.max(s, axis=1, keepdims=True))
            p = jnp.exp2(s - m_new[:, :1])
            if masked:
                p = jnp.where(allowed, p, 0.0)
            alpha = jnp.exp2(m_old - m_new)
            l_ref[h] = l_ref[h] * alpha + jnp.sum(p, axis=1, keepdims=True)
            acc_ref[h] = acc_ref[h] * alpha + jnp.dot(
                p.astype(jnp.bfloat16),
                v[:, h * VDIM : (h + 1) * VDIM],
                preferred_element_type=jnp.float32,
            )
            m_ref[h] = m_new

    @pl.when(i < whole)
    def _():
        step(False)

    @pl.when((i >= whole) & (i < needed))
    def _():
        step(True)

    @pl.when(i == nsteps - 1)
    def _():
        if last:
            for h in range(2):
                outs[0][:, h * VDIM : (h + 1) * VDIM] = (acc_ref[h] / l_ref[h]).astype(jnp.bfloat16)
        else:
            outs[0][...] = m_ref[...]
            outs[1][...] = l_ref[...]
            outs[2][...] = acc_ref[...]


def attend(q_cat, gathered, key_local, value_local, q_sp, core, state):
    first = state is None
    last = not first
    have = jnp.maximum((q_sp - core) // 2 + 1, 0)
    have = jnp.where(q_sp < core, 0, have)
    needed = (have + KB - 1) // KB
    full = jnp.where(q_sp <= core, 0, (q_sp - core + 1) // 2)
    whole = full // KB
    meta = jnp.stack([q_sp, core, needed, whole]).astype(jnp.int32)
    nsteps = (NZ * NX) // KB
    state_spec = pl.BlockSpec((2, ROWS, 128), lambda i, meta: (0, 0, 0))
    in_specs = [
        pl.BlockSpec((2, ROWS, 256), lambda i, meta: (0, 0, 0)),
        pl.BlockSpec(
            (KB, NY, PACK, 256),
            lambda i, meta: (jnp.minimum(i, jnp.maximum(meta[2] - 1, 0)), 0, 0, 0),
        ),
        pl.BlockSpec((256, 256), lambda i, meta: (0, 0)),
        pl.BlockSpec((256, 256), lambda i, meta: (0, 0)),
    ]
    args = [q_cat, gathered, key_local, value_local]
    if not first:
        in_specs += [state_spec] * 3
        args += list(state)
    if last:
        out_shape = jax.ShapeDtypeStruct((ROWS, 256), jnp.bfloat16)
        out_specs = pl.BlockSpec((ROWS, 256), lambda i, meta: (0, 0))
    else:
        out_shape = tuple(jax.ShapeDtypeStruct((2, ROWS, 128), jnp.float32) for _ in range(3))
        out_specs = (state_spec,) * 3
    import functools

    return pl.pallas_call(
        functools.partial(attend_kernel, first, last),
        out_shape=out_shape,
        grid_spec=pltpu.PrefetchScalarGridSpec(
            num_scalar_prefetch=1,
            grid=(nsteps,),
            in_specs=in_specs,
            out_specs=out_specs,
            scratch_shapes=[pltpu.VMEM((2, ROWS, 128), jnp.float32)] * 3,
        ),
        compiler_params=pltpu.CompilerParams(dimension_semantics=("arbitrary",)),
        cost_estimate=pl.CostEstimate(
            flops=3_000_000_000, bytes_accessed=6_000_000, transcendentals=4_000_000
        ),
    )(meta, *args)


def body(
    query_nope,
    query_rope,
    latent,
    key_rope,
    latent_gain,
    key_up,
    value_up,
    out_proj,
    residual,
    ffn_gain,
    expert_ids,
    route_weights,
    expert_gate,
    expert_up,
    expert_down,
    shared_gate,
    shared_up,
    shared_down,
):
    z, x, core, y = (lax.axis_index(n) for n in ("z", "x", "core", "y"))
    q_sp = (z * NX + x) * NC + core
    first_row = q_sp * ROWS
    positions = first_row + jnp.arange(ROWS, dtype=jnp.int32)

    lat_q = lax.dynamic_slice_in_dim(latent, y * QUART, QUART, 0)
    rope_q = lax.dynamic_slice_in_dim(key_rope, y * QUART, QUART, 0)
    pos_q = first_row + y * QUART + jnp.arange(QUART, dtype=jnp.int32)
    normed_latent = scale_rows(lat_q, latent_gain)
    rot_key = rotate(rope_q[:, None, :], pos_q)[:, 0, :]
    packed_rope = jnp.concatenate([rot_key[g * 16 : (g + 1) * 16] for g in range(4)], axis=1)
    payload = jnp.concatenate([normed_latent, packed_rope], axis=0)
    mine = lax.all_gather(payload, ("z", "x", "y"), axis=0, tiled=False)
    mine = mine.reshape(NZ * NX, NY, PACK, 256)
    theirs = lax.ppermute(mine, "core", [(0, 1), (1, 0)])

    key_local = lax.dynamic_slice_in_dim(key_up, y * 256, 256, 1)
    value_local = lax.dynamic_slice_in_dim(value_up, y * 256, 256, 1)
    rot_query = rotate(query_rope.reshape(ROWS, 2, ROPE), positions)
    q_cat = jnp.concatenate(
        [
            query_nope.reshape(ROWS, 2, NOPE),
            rot_query,
            jnp.zeros((ROWS, 2, 64), jnp.bfloat16),
        ],
        axis=-1,
    ).transpose(1, 0, 2)

    flat_ids = expert_ids.reshape(-1)
    onehot = (flat_ids[:, None] == jnp.arange(64, dtype=jnp.int32)[None, :]).astype(jnp.float32)
    earlier = (
        jnp.arange(256, dtype=jnp.int32)[None, :] < jnp.arange(256, dtype=jnp.int32)[:, None]
    ).astype(jnp.float32)
    before = jnp.dot(earlier, onehot)
    rank = jnp.sum(before * onehot, axis=1).reshape(64, 4)
    tables = jnp.concatenate([expert_ids.astype(jnp.float32) * CAP + rank, route_weights], axis=1)
    tables = lax.all_gather(tables, "z", axis=0, tiled=False)
    slot_of = tables[:, :, :4] - (z * 64).astype(jnp.float32)
    weight_of = tables[:, :, 4:]
    slots = jnp.arange(64, dtype=jnp.float32)
    hit = slot_of[:, :, :, None] == slots
    pick = jnp.any(hit, axis=2).astype(jnp.bfloat16)
    share = jnp.sum(jnp.where(hit, weight_of[:, :, :, None], 0.0), axis=2)
    share_hi = share.astype(jnp.bfloat16)
    share_lo = (share - share_hi.astype(jnp.float32)).astype(jnp.bfloat16)

    state = attend(q_cat, mine, key_local, value_local, q_sp, core, None)
    heads_out = attend(q_cat, theirs, key_local, value_local, q_sp, 1 - core, state)

    part = jnp.dot(heads_out, out_proj, preferred_element_type=jnp.float32).astype(jnp.bfloat16)
    pieces = lax.all_to_all(part.reshape(4, 64, 2048), "y", 0, 0, tiled=True)
    attn_sum = jnp.sum(pieces.astype(jnp.float32), axis=0)
    hidden_one = (residual.astype(jnp.float32) + attn_sum).astype(jnp.bfloat16)
    normed = scale_rows(hidden_one, ffn_gain)

    column = lax.all_gather(normed, "z", axis=0, tiled=False)
    outgoing = jnp.einsum(
        "stk,std->skd", pick, column, preferred_element_type=jnp.float32
    ).astype(jnp.bfloat16)
    outgoing = outgoing.reshape(8, 8, CAP, 2048).transpose(1, 0, 2, 3)
    arrived = lax.all_to_all(outgoing, ("x", "core"), split_axis=0, concat_axis=0, tiled=True)
    grouped = arrived.reshape(512, 2048)
    gate_part = jnp.dot(grouped, expert_gate[0], preferred_element_type=jnp.float32)
    upper_part = jnp.dot(grouped, expert_up[0], preferred_element_type=jnp.float32)
    expert_hidden = (jax.nn.silu(gate_part) * upper_part).astype(jnp.bfloat16)
    expert_rows = jnp.dot(
        expert_hidden, expert_down[0], preferred_element_type=jnp.float32
    ).astype(jnp.bfloat16)
    returned = lax.all_to_all(
        expert_rows.reshape(8, 8, CAP, 2048), ("x", "core"), split_axis=0, concat_axis=0, tiled=True
    )
    back = returned.transpose(1, 0, 2, 3).reshape(8, 64, 2048)
    partial = jnp.einsum("stk,skd->std", share_hi, back, preferred_element_type=jnp.float32)
    partial = partial + jnp.einsum(
        "stk,skd->std", share_lo, back, preferred_element_type=jnp.float32
    )
    routed = lax.psum_scatter(
        partial.astype(jnp.bfloat16), "z", scatter_dimension=0, tiled=False
    )

    shared_gate_part = jnp.dot(normed, shared_gate, preferred_element_type=jnp.float32)
    shared_upper = jnp.dot(normed, shared_up, preferred_element_type=jnp.float32)
    shared_hidden = (jax.nn.silu(shared_gate_part) * shared_upper).astype(jnp.bfloat16)
    shared_rows = jnp.dot(shared_hidden, shared_down, preferred_element_type=jnp.float32).astype(
        jnp.bfloat16
    )
    return (
        hidden_one.astype(jnp.float32)
        + routed.astype(jnp.float32)
        + shared_rows.astype(jnp.float32)
    ).astype(jnp.bfloat16)


def solution(mesh):
    fine = Mesh(mesh.devices.reshape(NZ, NX, NC, NY), ("z", "x", "core", "y"))
    sp = ("z", "x", "core")
    every = ("z", "x", "core", "y")
    in_specs = (
        P(sp, "y"),
        P(sp, "y"),
        P(sp, None),
        P(sp, None),
        P(),
        P(),
        P(),
        P("y", None),
        P(every, None),
        P(),
        P(every, None),
        P(every, None),
        P(sp, None, None),
        P(sp, None, None),
        P(sp, None, None),
        P(),
        P(),
        P(),
    )
    return jax.shard_map(
        body, mesh=fine, in_specs=in_specs, out_specs=P(every, None), check_vma=False
    )
```

```python
import math

import jax
import jax.numpy as jnp
from jax import lax
from jax.experimental import pallas as pl
from jax.experimental.pallas import tpu as pltpu
from jax.sharding import Mesh, PartitionSpec as P

NOPE = 128
ROPE = 64
VDIM = 128
NZ, NX, NC, NY = 8, 4, 2, 4
CAP = 8
ROWS = 256

rope_base = 10000.0
norm_eps = 1e-06


def scale_rows(values, gain_vec):
    as_float = values.astype(jnp.float32)
    factor = lax.rsqrt(jnp.mean(as_float * as_float, axis=-1, keepdims=True) + norm_eps)
    return (as_float * factor * gain_vec.astype(jnp.float32)).astype(jnp.bfloat16)


def rotate(values, positions):
    half_dim = values.shape[-1] // 2
    frequency = rope_base ** (-jnp.arange(half_dim, dtype=jnp.float32) / half_dim)
    angles = positions.astype(jnp.float32)[:, None, None] * frequency
    cosine = jnp.cos(angles)
    sine_part = jnp.sin(angles)
    as_float = values.astype(jnp.float32)
    first_half = as_float[..., :half_dim]
    second_half = as_float[..., half_dim:]
    return jnp.concatenate(
        [
            first_half * cosine - second_half * sine_part,
            first_half * sine_part + second_half * cosine,
        ],
        axis=-1,
    ).astype(jnp.bfloat16)


LOG2E = 1.4426950408889634
MESH_ID = pl.DeviceIdType.MESH
OFFS = (0, -1, 1, -2, 2, -3, 3, -4)
HALF = 160


def ring(value, size):
    return lax.rem(value + size, size)


def greet(partners):
    barrier = pltpu.get_barrier_semaphore()
    for dev in partners:
        pl.semaphore_signal(barrier, inc=1, device_id=dev, device_id_type=MESH_ID)
    pl.semaphore_wait(barrier, len(partners))


def gather_attend_kernel(
    pay_ref, tab_ref, q_ref, ku_ref, vu_ref, out_ref, tabs_ref,
    G, T, m_ref, l_ref, acc_ref, recv, trecv, zsend, tsend, xsend, fsend, ysend, csend, lsem,
):
    z, x, c, y = (lax.axis_index(n) for n in ("z", "x", "core", "y"))
    hm = lax.rem(y, 2)
    ho = 1 - hm
    up, down = {"z": ring(z + 1, NZ)}, {"z": ring(z - 1, NZ)}
    right, left = {"x": ring(x + 1, NX)}, {"x": ring(x - 1, NX)}
    above, below = {"y": ring(y + 1, NY)}, {"y": ring(y - 1, NY)}
    mate = {"core": 1 - c}
    xs = {0: x, -1: ring(x - 1, NX), 1: ring(x + 1, NX), 2: ring(x + 2, NX)}
    ZZ = [ring(z + off, NZ) for off in OFFS]
    greet([up, down, right, left, above, below, mate])

    def piece(zz, xx, h, sem, dev):
        slot = G.at[c, zz, xx, h]
        return pltpu.make_async_remote_copy(
            src_ref=slot, dst_ref=slot, send_sem=sem, recv_sem=recv.at[c, zz, xx, h],
            device_id=dev, device_id_type=MESH_ID,
        )

    def arrived(par, zz, xx, h):
        slot = G.at[par, zz, xx, h]
        pltpu.make_async_remote_copy(
            src_ref=slot, dst_ref=slot, send_sem=csend, recv_sem=recv.at[par, zz, xx, h],
            device_id=mate, device_id_type=MESH_ID,
        ).wait_recv()

    sent = []

    def send(zz, xx, h, sems, at, dev):
        piece(zz, xx, h, sems.at[at], dev).start()
        sent.append(lambda: piece(zz, xx, h, sems.at[at], dev).wait_send())

    def to_mate(zz, xx, h):
        piece(zz, xx, h, csend, mate).start()

    def table(zz, sem, dev):
        return pltpu.make_async_remote_copy(
            src_ref=T.at[zz], dst_ref=T.at[zz], send_sem=sem, recv_sem=trecv.at[zz],
            device_id=dev, device_id_type=MESH_ID,
        )

    def send_table(zz, at, dev):
        table(zz, tsend.at[at], dev).start()
        sent.append(lambda: table(zz, tsend.at[at], dev).wait_send())

    def ev_z(i):
        off = OFFS[i]
        zz = ZZ[i]
        for h in range(2):
            if i > 0:
                arrived(c, zz, x, h)
            if -4 < off <= 0:
                send(zz, x, h, zsend, (0, -off, h), up)
            if 0 <= off < 3:
                send(zz, x, h, zsend, (1, off, h), down)
            to_mate(zz, x, h)
        send(zz, x, hm, xsend, (i, 0), right)
        send(zz, x, hm, xsend, (i, 1), left)
        if i > 0:
            table(zz, tsend.at[0, 0], up).wait_recv()
        if -4 < off <= 0:
            send_table(zz, (0, -off), up)
        if 0 <= off < 3:
            send_table(zz, (1, off), down)

    def to_y(i, j, zz, xx):
        send(zz, xx, hm, ysend, (i, j), above if (i + j) % 2 == 0 else below)

    def ev_x1(i):
        zz = ZZ[i]
        arrived(c, zz, xs[-1], hm)
        if i % 2 == 0:
            send(zz, xs[-1], hm, fsend, (i,), right)
        to_y(i, 0, zz, xs[-1])
        to_mate(zz, xs[-1], hm)
        arrived(c, zz, xs[1], hm)
        if i % 2 == 1:
            send(zz, xs[1], hm, fsend, (i,), left)
        to_y(i, 1, zz, xs[1])
        to_mate(zz, xs[1], hm)

    def ev_x2(i):
        zz = ZZ[i]
        arrived(c, zz, xs[2], hm)
        to_y(i, 2, zz, xs[2])
        to_mate(zz, xs[2], hm)

    def ev_y(i, dx):
        zz = ZZ[i]
        arrived(c, zz, xs[dx], ho)
        to_mate(zz, xs[dx], ho)

    own = pltpu.make_async_copy(pay_ref, G.at[c, z, x], lsem.at[0])
    own_table = pltpu.make_async_copy(tab_ref, T.at[z], lsem.at[1])
    own.start()
    own_table.start()
    own.wait()
    own_table.wait()

    m_ref[...] = jnp.full(m_ref.shape, -1e30, jnp.float32)
    l_ref[...] = jnp.zeros(l_ref.shape, jnp.float32)
    acc_ref[...] = jnp.zeros(acc_ref.shape, jnp.float32)
    scale = LOG2E / math.sqrt(NOPE + ROPE)
    keys = 512

    def compute(zz, xx, masked):
        lat = jnp.concatenate(
            [G[par, zz, xx, h, 0:128, :] for par in range(2) for h in range(2)], axis=0
        )
        rope = jnp.concatenate(
            [
                G[par, zz, xx, h, 128:HALF, g * ROPE : (g + 1) * ROPE]
                for par in range(2)
                for h in range(2)
                for g in range(4)
            ],
            axis=0,
        )
        rope = jnp.concatenate([rope, jnp.zeros((keys, ROPE), jnp.bfloat16)], axis=1)
        k = jnp.dot(lat, ku_ref[...], preferred_element_type=jnp.float32).astype(jnp.bfloat16)
        v = jnp.dot(lat, vu_ref[...], preferred_element_type=jnp.float32).astype(jnp.bfloat16)
        if masked:
            kpos = lax.broadcasted_iota(jnp.int32, (1, keys), 1)
            qpos = c * ROWS + lax.broadcasted_iota(jnp.int32, (ROWS, 1), 0)
            allowed = kpos <= qpos
        for h in range(2):
            kcat = jnp.concatenate([k[:, h * NOPE : (h + 1) * NOPE], rope], axis=1)
            s = lax.dot_general(
                q_ref[h], kcat, (((1,), (1,)), ((), ())), preferred_element_type=jnp.float32
            )
            s = s * scale
            if masked:
                s = jnp.where(allowed, s, -1e30)
            m_old = m_ref[h]
            m_new = jnp.maximum(m_old, jnp.max(s, axis=1, keepdims=True))
            p = jnp.exp2(s - m_new[:, :1])
            if masked:
                p = jnp.where(allowed, p, 0.0)
            alpha = jnp.exp2(m_old - m_new)
            l_ref[h] = l_ref[h] * alpha + jnp.sum(p, axis=1, keepdims=True)
            acc_ref[h] = acc_ref[h] * alpha + jnp.dot(
                p.astype(jnp.bfloat16),
                v[:, h * VDIM : (h + 1) * VDIM],
                preferred_element_type=jnp.float32,
            )
            m_ref[h] = m_new

    mine = z * NX + x

    def round_(s, carry):
        for k in range(11):

            @pl.when(s == k)
            def _():
                if k < 8:
                    ev_z(k)
                if 0 <= k - 1 < 8:
                    ev_x1(k - 1)
                if 0 <= k - 2 < 8:
                    ev_x2(k - 2)
                    ev_y(k - 2, -1)
                    ev_y(k - 2, 1)
                if 0 <= k - 3 < 8:
                    ev_y(k - 3, 2)

        def pair(d, carry):
            i = s - 1 - jnp.where(d == 0, 0, jnp.where(d == 3, 3, 2))

            @pl.when((i >= 0) & (i < 8))
            def _():
                off = jnp.where(lax.rem(i, 2) == 1, -((i + 1) // 2), i // 2)
                dx = jnp.where(d == 3, 2, jnp.where(d == 1, -1, jnp.where(d == 2, 1, 0)))
                zz = ring(z + off, NZ)
                xx = ring(x + dx, NX)
                for h in range(2):
                    arrived(1 - c, zz, xx, h)
                theirs = zz * NX + xx

                @pl.when(theirs < mine)
                def _():
                    compute(zz, xx, False)

                @pl.when(theirs == mine)
                def _():
                    compute(zz, xx, True)

            return carry

        return lax.fori_loop(0, 4, pair, carry)

    lax.fori_loop(0, 12, round_, 0)

    for h in range(2):
        out_ref[:, h * VDIM : (h + 1) * VDIM] = (acc_ref[h] / l_ref[h]).astype(jnp.bfloat16)
    tabs_ref[...] = T[...]
    for wait in sent:
        wait()
    whole = G.at[c]
    pltpu.make_async_remote_copy(
        src_ref=whole, dst_ref=whole, send_sem=csend, recv_sem=recv.at[0, 0, 0, 0],
        device_id=mate, device_id_type=MESH_ID,
    ).wait_send()


def gather_attend(payload, tables, q_cat, key_local, value_local):
    vmem = pl.BlockSpec(memory_space=pltpu.VMEM)
    return pl.pallas_call(
        gather_attend_kernel,
        out_shape=(
            jax.ShapeDtypeStruct((ROWS, 256), jnp.bfloat16),
            jax.ShapeDtypeStruct((NZ, 8, 128), jnp.float32),
        ),
        in_specs=[vmem] * 5,
        out_specs=(vmem, vmem),
        scratch_shapes=[
            pltpu.VMEM((2, NZ, NX, 2, HALF, 256), jnp.bfloat16),
            pltpu.VMEM((NZ, 8, 128), jnp.float32),
            pltpu.VMEM((2, ROWS, 128), jnp.float32),
            pltpu.VMEM((2, ROWS, 128), jnp.float32),
            pltpu.VMEM((2, ROWS, 128), jnp.float32),
            pltpu.SemaphoreType.DMA((2, NZ, NX, 2)),
            pltpu.SemaphoreType.DMA((NZ,)),
            pltpu.SemaphoreType.DMA((2, 4, 2)),
            pltpu.SemaphoreType.DMA((2, 4)),
            pltpu.SemaphoreType.DMA((8, 2)),
            pltpu.SemaphoreType.DMA((8,)),
            pltpu.SemaphoreType.DMA((8, 3)),
            pltpu.SemaphoreType.DMA,
            pltpu.SemaphoreType.DMA((2,)),
        ],
        compiler_params=pltpu.CompilerParams(
            collective_id=0, has_side_effects=True, vmem_limit_bytes=40 * 1024 * 1024
        ),
    )(payload, tables, q_cat, key_local, value_local)


def body(
    query_nope,
    query_rope,
    latent,
    key_rope,
    latent_gain,
    key_up,
    value_up,
    out_proj,
    residual,
    ffn_gain,
    expert_ids,
    route_weights,
    expert_gate,
    expert_up,
    expert_down,
    shared_gate,
    shared_up,
    shared_down,
):
    z, x, core, y = (lax.axis_index(n) for n in ("z", "x", "core", "y"))
    q_sp = (z * NX + x) * NC + core
    first_row = q_sp * ROWS
    positions = first_row + jnp.arange(ROWS, dtype=jnp.int32)

    normed_latent = scale_rows(latent, latent_gain)
    rot_key = rotate(key_rope[:, None, :], positions)[:, 0, :]
    packed = rot_key.reshape(2, 4, 32, ROPE).transpose(0, 2, 1, 3).reshape(2, 32, 256)
    payload = jnp.concatenate([normed_latent.reshape(2, 128, 256), packed], axis=1)

    key_local = lax.dynamic_slice_in_dim(key_up, y * 256, 256, 1)
    value_local = lax.dynamic_slice_in_dim(value_up, y * 256, 256, 1)
    rot_query = rotate(query_rope.reshape(ROWS, 2, ROPE), positions)
    q_cat = jnp.concatenate(
        [
            query_nope.reshape(ROWS, 2, NOPE),
            rot_query,
            jnp.zeros((ROWS, 2, 64), jnp.bfloat16),
        ],
        axis=-1,
    ).transpose(1, 0, 2)

    flat_ids = expert_ids.reshape(-1)
    onehot = (flat_ids[:, None] == jnp.arange(64, dtype=jnp.int32)[None, :]).astype(jnp.float32)
    earlier = (
        jnp.arange(256, dtype=jnp.int32)[None, :] < jnp.arange(256, dtype=jnp.int32)[:, None]
    ).astype(jnp.float32)
    before = jnp.dot(earlier, onehot)
    rank = jnp.sum(before * onehot, axis=1).reshape(64, 4)
    tables = jnp.concatenate([expert_ids.astype(jnp.float32) * CAP + rank, route_weights], axis=1)
    tables = jnp.concatenate([tables.T, jnp.zeros((8, 64), jnp.float32)], axis=1)
    heads_out, gathered = gather_attend(payload, tables, q_cat, key_local, value_local)
    tables = gathered[:, :, :64].transpose(0, 2, 1)
    slot_of = tables[:, :, :4] - (z * 64).astype(jnp.float32)
    weight_of = tables[:, :, 4:]
    slots = jnp.arange(64, dtype=jnp.float32)
    hit = slot_of[:, :, :, None] == slots
    pick = jnp.any(hit, axis=2).astype(jnp.bfloat16)
    share = jnp.sum(jnp.where(hit, weight_of[:, :, :, None], 0.0), axis=2)
    share_hi = share.astype(jnp.bfloat16)
    share_lo = (share - share_hi.astype(jnp.float32)).astype(jnp.bfloat16)

    part = jnp.dot(heads_out, out_proj, preferred_element_type=jnp.float32).astype(jnp.bfloat16)
    pieces = lax.all_to_all(part.reshape(4, 64, 2048), "y", 0, 0, tiled=True)
    attn_sum = jnp.sum(pieces.astype(jnp.float32), axis=0)
    hidden_one = (residual.astype(jnp.float32) + attn_sum).astype(jnp.bfloat16)
    normed = scale_rows(hidden_one, ffn_gain)

    column = lax.all_gather(normed, "z", axis=0, tiled=False)
    outgoing = jnp.einsum(
        "stk,std->skd", pick, column, preferred_element_type=jnp.float32
    ).astype(jnp.bfloat16)
    outgoing = outgoing.reshape(8, 8, CAP, 2048).transpose(1, 0, 2, 3)
    arrived = lax.all_to_all(outgoing, ("x", "core"), split_axis=0, concat_axis=0, tiled=True)
    grouped = arrived.reshape(512, 2048)
    gate_part = jnp.dot(grouped, expert_gate[0], preferred_element_type=jnp.float32)
    upper_part = jnp.dot(grouped, expert_up[0], preferred_element_type=jnp.float32)
    expert_hidden = (jax.nn.silu(gate_part) * upper_part).astype(jnp.bfloat16)
    expert_rows = jnp.dot(
        expert_hidden, expert_down[0], preferred_element_type=jnp.float32
    ).astype(jnp.bfloat16)
    returned = lax.all_to_all(
        expert_rows.reshape(8, 8, CAP, 2048), ("x", "core"), split_axis=0, concat_axis=0, tiled=True
    )
    back = returned.transpose(1, 0, 2, 3).reshape(8, 64, 2048)
    partial = jnp.einsum("stk,skd->std", share_hi, back, preferred_element_type=jnp.float32)
    partial = partial + jnp.einsum(
        "stk,skd->std", share_lo, back, preferred_element_type=jnp.float32
    )
    routed = lax.psum_scatter(
        partial.astype(jnp.bfloat16), "z", scatter_dimension=0, tiled=False
    )

    shared_gate_part = jnp.dot(normed, shared_gate, preferred_element_type=jnp.float32)
    shared_upper = jnp.dot(normed, shared_up, preferred_element_type=jnp.float32)
    shared_hidden = (jax.nn.silu(shared_gate_part) * shared_upper).astype(jnp.bfloat16)
    shared_rows = jnp.dot(shared_hidden, shared_down, preferred_element_type=jnp.float32).astype(
        jnp.bfloat16
    )
    return (
        hidden_one.astype(jnp.float32)
        + routed.astype(jnp.float32)
        + shared_rows.astype(jnp.float32)
    ).astype(jnp.bfloat16)


def solution(mesh):
    fine = Mesh(mesh.devices.reshape(NZ, NX, NC, NY), ("z", "x", "core", "y"))
    sp = ("z", "x", "core")
    every = ("z", "x", "core", "y")
    in_specs = (
        P(sp, "y"),
        P(sp, "y"),
        P(sp, None),
        P(sp, None),
        P(),
        P(),
        P(),
        P("y", None),
        P(every, None),
        P(),
        P(every, None),
        P(every, None),
        P(sp, None, None),
        P(sp, None, None),
        P(sp, None, None),
        P(),
        P(),
        P(),
    )
    return jax.shard_map(
        body, mesh=fine, in_specs=in_specs, out_specs=P(every, None), check_vma=False
    )
```

```python
import math

import jax
import jax.numpy as jnp
from jax import lax
from jax.experimental import pallas as pl
from jax.experimental.pallas import tpu as pltpu
from jax.sharding import Mesh, PartitionSpec as P

NOPE = 128
ROPE = 64
VDIM = 128
NZ, NX, NC, NY = 8, 4, 2, 4
CAP = 8
ROWS = 256

rope_base = 10000.0
norm_eps = 1e-06


def scale_rows(values, gain_vec):
    as_float = values.astype(jnp.float32)
    factor = lax.rsqrt(jnp.mean(as_float * as_float, axis=-1, keepdims=True) + norm_eps)
    return (as_float * factor * gain_vec.astype(jnp.float32)).astype(jnp.bfloat16)


def rotate(values, positions):
    half_dim = values.shape[-1] // 2
    frequency = rope_base ** (-jnp.arange(half_dim, dtype=jnp.float32) / half_dim)
    angles = positions.astype(jnp.float32)[:, None, None] * frequency
    cosine = jnp.cos(angles)
    sine_part = jnp.sin(angles)
    as_float = values.astype(jnp.float32)
    first_half = as_float[..., :half_dim]
    second_half = as_float[..., half_dim:]
    return jnp.concatenate(
        [
            first_half * cosine - second_half * sine_part,
            first_half * sine_part + second_half * cosine,
        ],
        axis=-1,
    ).astype(jnp.bfloat16)


LOG2E = 1.4426950408889634
MESH_ID = pl.DeviceIdType.MESH
OFFS = (0, -1, 1, -2, 2, -3, 3, -4)
HALF = 160


def ring(value, size):
    return lax.rem(value + size, size)


def greet(partners):
    barrier = pltpu.get_barrier_semaphore()
    for dev in partners:
        pl.semaphore_signal(barrier, inc=1, device_id=dev, device_id_type=MESH_ID)
    pl.semaphore_wait(barrier, len(partners))


def gather_attend_kernel(
    pay_ref, tab_ref, q_ref, ku_ref, vu_ref, out_ref, tabs_ref,
    G, T, m_ref, l_ref, acc_ref, recv, trecv, zsend, tsend, xsend, fsend, ysend, csend, lsem,
):
    z, x, c, y = (lax.axis_index(n) for n in ("z", "x", "core", "y"))
    hm = lax.rem(y, 2)
    ho = 1 - hm
    up, down = {"z": ring(z + 1, NZ)}, {"z": ring(z - 1, NZ)}
    right, left = {"x": ring(x + 1, NX)}, {"x": ring(x - 1, NX)}
    above, below = {"y": ring(y + 1, NY)}, {"y": ring(y - 1, NY)}
    mate = {"core": 1 - c}
    xs = {0: x, -1: ring(x - 1, NX), 1: ring(x + 1, NX), 2: ring(x + 2, NX)}
    ZZ = [ring(z + off, NZ) for off in OFFS]
    greet([up, down, right, left, above, below, mate])

    def piece(zz, xx, h, sem, dev):
        slot = G.at[c, zz, xx, h]
        return pltpu.make_async_remote_copy(
            src_ref=slot, dst_ref=slot, send_sem=sem, recv_sem=recv.at[c, zz, xx, h],
            device_id=dev, device_id_type=MESH_ID,
        )

    def arrived(par, zz, xx, h):
        slot = G.at[par, zz, xx, h]
        pltpu.make_async_remote_copy(
            src_ref=slot, dst_ref=slot, send_sem=csend, recv_sem=recv.at[par, zz, xx, h],
            device_id=mate, device_id_type=MESH_ID,
        ).wait_recv()

    sent = []

    def send(zz, xx, h, sems, at, dev):
        piece(zz, xx, h, sems.at[at], dev).start()
        sent.append(lambda: piece(zz, xx, h, sems.at[at], dev).wait_send())

    def to_mate(zz, xx, h):
        piece(zz, xx, h, csend, mate).start()

    def table(zz, sem, dev):
        return pltpu.make_async_remote_copy(
            src_ref=T.at[zz], dst_ref=T.at[zz], send_sem=sem, recv_sem=trecv.at[zz],
            device_id=dev, device_id_type=MESH_ID,
        )

    def send_table(zz, at, dev):
        table(zz, tsend.at[at], dev).start()
        sent.append(lambda: table(zz, tsend.at[at], dev).wait_send())

    def ev_z(i):
        off = OFFS[i]
        zz = ZZ[i]
        for h in range(2):
            if i > 0:
                arrived(c, zz, x, h)
            if -4 < off <= 0:
                send(zz, x, h, zsend, (0, -off, h), up)
            if 0 <= off < 3:
                send(zz, x, h, zsend, (1, off, h), down)
            to_mate(zz, x, h)
        send(zz, x, hm, xsend, (i, 0), right)
        send(zz, x, hm, xsend, (i, 1), left)
        if i > 0:
            table(zz, tsend.at[0, 0], up).wait_recv()
        if -4 < off <= 0:
            send_table(zz, (0, -off), up)
        if 0 <= off < 3:
            send_table(zz, (1, off), down)

    def to_y(i, j, zz, xx):
        send(zz, xx, hm, ysend, (i, j), above if (i + j) % 2 == 0 else below)

    def ev_x1(i):
        zz = ZZ[i]
        arrived(c, zz, xs[-1], hm)
        if i % 2 == 0:
            send(zz, xs[-1], hm, fsend, (i,), right)
        to_y(i, 0, zz, xs[-1])
        to_mate(zz, xs[-1], hm)
        arrived(c, zz, xs[1], hm)
        if i % 2 == 1:
            send(zz, xs[1], hm, fsend, (i,), left)
        to_y(i, 1, zz, xs[1])
        to_mate(zz, xs[1], hm)

    def ev_x2(i):
        zz = ZZ[i]
        arrived(c, zz, xs[2], hm)
        to_y(i, 2, zz, xs[2])
        to_mate(zz, xs[2], hm)

    def ev_y(i, dx):
        zz = ZZ[i]
        arrived(c, zz, xs[dx], ho)
        to_mate(zz, xs[dx], ho)

    own = pltpu.make_async_copy(pay_ref, G.at[c, z, x], lsem.at[0])
    own_table = pltpu.make_async_copy(tab_ref, T.at[z], lsem.at[1])
    own.start()
    own_table.start()
    own.wait()
    own_table.wait()

    m_ref[...] = jnp.full(m_ref.shape, -1e30, jnp.float32)
    l_ref[...] = jnp.zeros(l_ref.shape, jnp.float32)
    acc_ref[...] = jnp.zeros(acc_ref.shape, jnp.float32)
    scale = LOG2E / math.sqrt(NOPE + ROPE)
    keys = 512

    def compute(zz, xx, masked):
        lat = jnp.concatenate(
            [G[par, zz, xx, h, 0:128, :] for par in range(2) for h in range(2)], axis=0
        )
        rope = jnp.concatenate(
            [
                G[par, zz, xx, h, 128:HALF, g * ROPE : (g + 1) * ROPE]
                for par in range(2)
                for h in range(2)
                for g in range(4)
            ],
            axis=0,
        )
        rope = jnp.concatenate([rope, jnp.zeros((keys, ROPE), jnp.bfloat16)], axis=1)
        k = jnp.dot(lat, ku_ref[...], preferred_element_type=jnp.float32).astype(jnp.bfloat16)
        v = jnp.dot(lat, vu_ref[...], preferred_element_type=jnp.float32).astype(jnp.bfloat16)
        if masked:
            kpos = lax.broadcasted_iota(jnp.int32, (1, keys), 1)
            qpos = c * ROWS + lax.broadcasted_iota(jnp.int32, (ROWS, 1), 0)
            allowed = kpos <= qpos
        for h in range(2):
            kcat = jnp.concatenate([k[:, h * NOPE : (h + 1) * NOPE], rope], axis=1)
            s = lax.dot_general(
                q_ref[h], kcat, (((1,), (1,)), ((), ())), preferred_element_type=jnp.float32
            )
            s = s * scale
            if masked:
                s = jnp.where(allowed, s, -1e30)
            m_old = m_ref[h]
            m_new = jnp.maximum(m_old, jnp.max(s, axis=1, keepdims=True))
            p = jnp.exp2(s - m_new[:, :1])
            if masked:
                p = jnp.where(allowed, p, 0.0)
            alpha = jnp.exp2(m_old - m_new)
            l_ref[h] = l_ref[h] * alpha + jnp.sum(p, axis=1, keepdims=True)
            acc_ref[h] = acc_ref[h] * alpha + jnp.dot(
                p.astype(jnp.bfloat16),
                v[:, h * VDIM : (h + 1) * VDIM],
                preferred_element_type=jnp.float32,
            )
            m_ref[h] = m_new

    mine = z * NX + x

    def round_(s, carry):
        for k in range(11):

            @pl.when(s == k)
            def _():
                if k < 8:
                    ev_z(k)
                if 0 <= k - 1 < 8:
                    ev_x1(k - 1)
                if 0 <= k - 2 < 8:
                    ev_x2(k - 2)
                    ev_y(k - 2, -1)
                    ev_y(k - 2, 1)
                if 0 <= k - 3 < 8:
                    ev_y(k - 3, 2)

        def pair(d, carry):
            i = s - 1 - jnp.where(d == 0, 0, jnp.where(d == 3, 3, 2))

            @pl.when((i >= 0) & (i < 8))
            def _():
                off = jnp.where(lax.rem(i, 2) == 1, -((i + 1) // 2), i // 2)
                dx = jnp.where(d == 3, 2, jnp.where(d == 1, -1, jnp.where(d == 2, 1, 0)))
                zz = ring(z + off, NZ)
                xx = ring(x + dx, NX)
                for h in range(2):
                    arrived(1 - c, zz, xx, h)
                theirs = zz * NX + xx

                @pl.when(theirs < mine)
                def _():
                    compute(zz, xx, False)

                @pl.when(theirs == mine)
                def _():
                    compute(zz, xx, True)

            return carry

        return lax.fori_loop(0, 4, pair, carry)

    lax.fori_loop(0, 12, round_, 0)

    for h in range(2):
        out_ref[:, h * VDIM : (h + 1) * VDIM] = (acc_ref[h] / l_ref[h]).astype(jnp.bfloat16)
    tabs_ref[...] = T[...]
    for wait in sent:
        wait()
    whole = G.at[c]
    pltpu.make_async_remote_copy(
        src_ref=whole, dst_ref=whole, send_sem=csend, recv_sem=recv.at[0, 0, 0, 0],
        device_id=mate, device_id_type=MESH_ID,
    ).wait_send()


def gather_attend(payload, tables, q_cat, key_local, value_local):
    vmem = pl.BlockSpec(memory_space=pltpu.VMEM)
    return pl.pallas_call(
        gather_attend_kernel,
        out_shape=(
            jax.ShapeDtypeStruct((ROWS, 256), jnp.bfloat16),
            jax.ShapeDtypeStruct((NZ, 8, 128), jnp.float32),
        ),
        in_specs=[vmem] * 5,
        out_specs=(vmem, vmem),
        scratch_shapes=[
            pltpu.VMEM((2, NZ, NX, 2, HALF, 256), jnp.bfloat16),
            pltpu.VMEM((NZ, 8, 128), jnp.float32),
            pltpu.VMEM((2, ROWS, 128), jnp.float32),
            pltpu.VMEM((2, ROWS, 128), jnp.float32),
            pltpu.VMEM((2, ROWS, 128), jnp.float32),
            pltpu.SemaphoreType.DMA((2, NZ, NX, 2)),
            pltpu.SemaphoreType.DMA((NZ,)),
            pltpu.SemaphoreType.DMA((2, 4, 2)),
            pltpu.SemaphoreType.DMA((2, 4)),
            pltpu.SemaphoreType.DMA((8, 2)),
            pltpu.SemaphoreType.DMA((8,)),
            pltpu.SemaphoreType.DMA((8, 3)),
            pltpu.SemaphoreType.DMA,
            pltpu.SemaphoreType.DMA((2,)),
        ],
        compiler_params=pltpu.CompilerParams(
            collective_id=0, has_side_effects=True, vmem_limit_bytes=40 * 1024 * 1024
        ),
    )(payload, tables, q_cat, key_local, value_local)


def moe_kernel(
    norm_ref, hid_ref, tab_ref, wg_h, wu_h, wd_h, sg_h, su_h, sd_h, out_ref,
    COL, OUT, ARR, EO, RET, PART, RD, RU, wg, wu, wd, sg, su, sd,
    zrecv, zsend, arecv, asend, rrecv, rsend, drecv, dsend, lsem, wsem,
):
    z, x, c, y = (lax.axis_index(n) for n in ("z", "x", "core", "y"))
    me = x * NC + c
    up, down = {"z": ring(z + 1, NZ)}, {"z": ring(z - 1, NZ)}
    peers = []
    for q in range(1, 8):
        p = ring(me + q, 8)
        peers.append((p, {"x": p // NC, "core": lax.rem(p, NC)}))

    weights = [
        pltpu.make_async_copy(src, dst, wsem.at[n])
        for n, (src, dst) in enumerate(
            ((sg_h, sg), (su_h, su), (sd_h, sd), (wg_h, wg), (wu_h, wu), (wd_h, wd))
        )
    ]
    own = pltpu.make_async_copy(norm_ref, COL.at[0], lsem.at[0])
    own.start()
    for w in weights:
        w.start()
    greet([up, down] + [dev for _, dev in peers])
    own.wait()

    at = {off: i for i, off in enumerate(OFFS)}

    def along_z(i, dev, off_to, sems, n):
        return pltpu.make_async_remote_copy(
            src_ref=COL.at[i], dst_ref=COL.at[at[off_to]], send_sem=sems.at[n],
            recv_sem=zrecv.at[at[off_to]], device_id=dev, device_id_type=MESH_ID,
        )

    sends = []

    def start(copy):
        copy.start()
        sends.append(copy)

    def pieces(i, src, dst, sems_send, sems_recv):
        for p, dev in peers:
            pltpu.make_async_remote_copy(
                src_ref=src.at[i, p], dst_ref=dst.at[i, me], send_sem=sems_send.at[i],
                recv_sem=sems_recv.at[i], device_id=dev, device_id_type=MESH_ID,
            ).start()
        pltpu.make_async_copy(src.at[i, me], dst.at[i, me], lsem.at[1]).start()
        pltpu.make_async_copy(src.at[i, me], dst.at[i, me], lsem.at[1]).wait()

    def pieces_in(i, dst, sems_recv):
        ref = dst.at[i, 0:7]
        pltpu.make_async_remote_copy(
            src_ref=ref, dst_ref=ref, send_sem=lsem.at[2], recv_sem=sems_recv.at[i],
            device_id=peers[0][1], device_id_type=MESH_ID,
        ).wait_recv()

    def pieces_sent(i, src, sems_send):
        ref = src.at[i, 0:7]
        pltpu.make_async_remote_copy(
            src_ref=ref, dst_ref=ref, send_sem=sems_send.at[i], recv_sem=lsem.at[2],
            device_id=peers[0][1], device_id_type=MESH_ID,
        ).wait_send()

    slots = lax.broadcasted_iota(jnp.int32, (64, 64), 0).astype(jnp.float32)

    def matches(i):
        tab = tab_ref[ring(z + OFFS[i], NZ)]
        base = (z * 64).astype(jnp.float32)
        return [(tab[k : k + 1, 0:64] - base) == slots for k in range(4)], tab

    def arrive(i):
        off = OFFS[i]
        if i > 0:
            along_z(i, up, off, zsend, 0).wait_recv()
        if -4 < off <= 0:
            start(along_z(i, up, off - 1, zsend, -off))
        if 0 <= off < 3:
            start(along_z(i, down, off + 1, zsend, 4 + off))
        hit, _ = matches(i)
        pick = jnp.where(hit[0] | hit[1] | hit[2] | hit[3], 1.0, 0.0).astype(jnp.bfloat16)
        rows = jnp.dot(pick, COL[i], preferred_element_type=jnp.float32)
        for p in range(8):
            OUT[i, p] = rows[p * CAP : (p + 1) * CAP].astype(jnp.bfloat16)
        pieces(i, OUT, ARR, asend, arecv)

    def gated(rows, gate, upper, lower):
        g = jnp.dot(rows, gate[...], preferred_element_type=jnp.float32)
        u = jnp.dot(rows, upper[...], preferred_element_type=jnp.float32)
        hidden = (g / (1.0 + jnp.exp(-g)) * u).astype(jnp.bfloat16)
        return jnp.dot(hidden, lower[...], preferred_element_type=jnp.float32)

    def expert(group):
        for i in group:
            pieces_in(i, ARR, arecv)
        rows = jnp.concatenate(
            [ARR[i, p].astype(jnp.float32) for i in group for p in range(8)], axis=0
        ).astype(jnp.bfloat16)
        done = gated(rows, wg, wu, wd)
        for n, i in enumerate(group):
            for p in range(8):
                lo = (n * 8 + p) * CAP
                EO[i, p] = done[lo : lo + CAP].astype(jnp.bfloat16)
            pieces(i, EO, RET, rsend, rrecv)

    def combine(i):
        pieces_in(i, RET, rrecv)
        hit, tab = matches(i)
        share = jnp.zeros((64, 64), jnp.float32)
        for k in range(4):
            share = share + jnp.where(hit[k], tab[4 + k : 5 + k, 0:64], 0.0)
        hi = share.astype(jnp.bfloat16)
        lo = (share - hi.astype(jnp.float32)).astype(jnp.bfloat16)
        back = jnp.concatenate(
            [RET[i, p].astype(jnp.float32) for p in range(8)], axis=0
        ).astype(jnp.bfloat16)
        dims = (((0,), (0,)), ((), ()))
        total = lax.dot_general(hi, back, dims, preferred_element_type=jnp.float32)
        total = total + lax.dot_general(lo, back, dims, preferred_element_type=jnp.float32)
        PART[i] = total.astype(jnp.bfloat16)

    groups = ((0,), (1, 2), (3, 4), (5, 6), (7,))
    for s in range(7):
        if s < 5:
            for i in groups[s]:
                arrive(i)
        if s == 0:
            for w in weights[:3]:
                w.wait()
            out_ref[...] = (
                hid_ref[...].astype(jnp.float32)
                + gated(norm_ref[...], sg, su, sd).astype(jnp.bfloat16).astype(jnp.float32)
            )
            for w in weights[3:]:
                w.wait()
        if 0 <= s - 1 < 5:
            expert(groups[s - 1])
        if 0 <= s - 2 < 5:
            for i in groups[s - 2]:
                combine(i)

    def back_z(src, dst, n, dev):
        return pltpu.make_async_remote_copy(
            src_ref=src, dst_ref=dst.at[n], send_sem=dsend.at[0 if dst is RD else 1, n],
            recv_sem=drecv.at[0 if dst is RD else 1, n], device_id=dev, device_id_type=MESH_ID,
        )

    start(back_z(PART.at[at[-4]], RD, 3, down))
    start(back_z(PART.at[at[3]], RU, 2, up))
    for k in (3, 2, 1):
        copy = back_z(PART.at[at[-k]], RD, k, down)
        copy.wait_recv()
        PART[at[-k]] = (
            PART[at[-k]].astype(jnp.float32) + RD[k].astype(jnp.float32)
        ).astype(jnp.bfloat16)
        start(back_z(PART.at[at[-k]], RD, k - 1, down))
        if k < 3:
            back_z(PART.at[at[k]], RU, k, up).wait_recv()
            PART[at[k]] = (
                PART[at[k]].astype(jnp.float32) + RU[k].astype(jnp.float32)
            ).astype(jnp.bfloat16)
            start(back_z(PART.at[at[k]], RU, k - 1, up))
    back_z(PART.at[0], RD, 0, down).wait_recv()
    back_z(PART.at[0], RU, 0, up).wait_recv()
    routed = PART[0].astype(jnp.float32) + RD[0].astype(jnp.float32) + RU[0].astype(jnp.float32)
    out_ref[...] = out_ref[...] + routed.astype(jnp.bfloat16).astype(jnp.float32)

    for copy in sends:
        copy.wait_send()
    for i in range(8):
        pieces_sent(i, OUT, asend)
        pieces_sent(i, EO, rsend)


def experts_layer(normed, hidden, tables, wg, wu, wd, sg, su, sd):
    vmem = pl.BlockSpec(memory_space=pltpu.VMEM)
    hbm = pl.BlockSpec(memory_space=pl.ANY)
    d, f = wg.shape
    bf = jnp.bfloat16
    return pl.pallas_call(
        moe_kernel,
        out_shape=jax.ShapeDtypeStruct((64, d), jnp.float32),
        in_specs=[vmem] * 3 + [hbm] * 6,
        out_specs=vmem,
        scratch_shapes=[
            pltpu.VMEM((8, 64, d), bf),
            pltpu.VMEM((8, 8, CAP, d), bf),
            pltpu.VMEM((8, 8, CAP, d), bf),
            pltpu.VMEM((8, 8, CAP, d), bf),
            pltpu.VMEM((8, 8, CAP, d), bf),
            pltpu.VMEM((8, 64, d), bf),
            pltpu.VMEM((4, 64, d), bf),
            pltpu.VMEM((3, 64, d), bf),
            pltpu.VMEM((d, f), bf),
            pltpu.VMEM((d, f), bf),
            pltpu.VMEM((f, d), bf),
            pltpu.VMEM((d, f), bf),
            pltpu.VMEM((d, f), bf),
            pltpu.VMEM((f, d), bf),
            pltpu.SemaphoreType.DMA((8,)),
            pltpu.SemaphoreType.DMA((8,)),
            pltpu.SemaphoreType.DMA((8,)),
            pltpu.SemaphoreType.DMA((8,)),
            pltpu.SemaphoreType.DMA((8,)),
            pltpu.SemaphoreType.DMA((8,)),
            pltpu.SemaphoreType.DMA((2, 4)),
            pltpu.SemaphoreType.DMA((2, 4)),
            pltpu.SemaphoreType.DMA((3,)),
            pltpu.SemaphoreType.DMA((6,)),
        ],
        compiler_params=pltpu.CompilerParams(
            collective_id=1, has_side_effects=True, vmem_limit_bytes=48 * 1024 * 1024
        ),
    )(normed, hidden, tables, wg, wu, wd, sg, su, sd)


def body(
    query_nope,
    query_rope,
    latent,
    key_rope,
    latent_gain,
    key_up,
    value_up,
    out_proj,
    residual,
    ffn_gain,
    expert_ids,
    route_weights,
    expert_gate,
    expert_up,
    expert_down,
    shared_gate,
    shared_up,
    shared_down,
):
    z, x, core, y = (lax.axis_index(n) for n in ("z", "x", "core", "y"))
    q_sp = (z * NX + x) * NC + core
    first_row = q_sp * ROWS
    positions = first_row + jnp.arange(ROWS, dtype=jnp.int32)

    normed_latent = scale_rows(latent, latent_gain)
    rot_key = rotate(key_rope[:, None, :], positions)[:, 0, :]
    packed = rot_key.reshape(2, 4, 32, ROPE).transpose(0, 2, 1, 3).reshape(2, 32, 256)
    payload = jnp.concatenate([normed_latent.reshape(2, 128, 256), packed], axis=1)

    key_local = lax.dynamic_slice_in_dim(key_up, y * 256, 256, 1)
    value_local = lax.dynamic_slice_in_dim(value_up, y * 256, 256, 1)
    rot_query = rotate(query_rope.reshape(ROWS, 2, ROPE), positions)
    q_cat = jnp.concatenate(
        [
            query_nope.reshape(ROWS, 2, NOPE),
            rot_query,
            jnp.zeros((ROWS, 2, 64), jnp.bfloat16),
        ],
        axis=-1,
    ).transpose(1, 0, 2)

    flat_ids = expert_ids.reshape(-1)
    onehot = (flat_ids[:, None] == jnp.arange(64, dtype=jnp.int32)[None, :]).astype(jnp.float32)
    earlier = (
        jnp.arange(256, dtype=jnp.int32)[None, :] < jnp.arange(256, dtype=jnp.int32)[:, None]
    ).astype(jnp.float32)
    before = jnp.dot(earlier, onehot)
    rank = jnp.sum(before * onehot, axis=1).reshape(64, 4)
    tables = jnp.concatenate([expert_ids.astype(jnp.float32) * CAP + rank, route_weights], axis=1)
    tables = jnp.concatenate([tables.T, jnp.zeros((8, 64), jnp.float32)], axis=1)
    heads_out, gathered = gather_attend(payload, tables, q_cat, key_local, value_local)
    part = jnp.dot(heads_out, out_proj, preferred_element_type=jnp.float32).astype(jnp.bfloat16)
    pieces = lax.all_to_all(part.reshape(4, 64, 2048), "y", 0, 0, tiled=True)
    attn_sum = jnp.sum(pieces.astype(jnp.float32), axis=0)
    hidden_one = (residual.astype(jnp.float32) + attn_sum).astype(jnp.bfloat16)
    normed = scale_rows(hidden_one, ffn_gain)

    summed = experts_layer(
        normed, hidden_one, gathered, expert_gate[0], expert_up[0], expert_down[0],
        shared_gate, shared_up, shared_down,
    )
    return summed.astype(jnp.bfloat16)


def solution(mesh):
    fine = Mesh(mesh.devices.reshape(NZ, NX, NC, NY), ("z", "x", "core", "y"))
    sp = ("z", "x", "core")
    every = ("z", "x", "core", "y")
    in_specs = (
        P(sp, "y"),
        P(sp, "y"),
        P(sp, None),
        P(sp, None),
        P(),
        P(),
        P(),
        P("y", None),
        P(every, None),
        P(),
        P(every, None),
        P(every, None),
        P(sp, None, None),
        P(sp, None, None),
        P(sp, None, None),
        P(),
        P(),
        P(),
    )
    return jax.shard_map(
        body, mesh=fine, in_specs=in_specs, out_specs=P(every, None), check_vma=False
    )
```

```python
import math

import jax
import jax.numpy as jnp
from jax import lax
from jax.experimental import pallas as pl
from jax.experimental.pallas import tpu as pltpu
from jax.sharding import Mesh, PartitionSpec as P

NOPE = 128
ROPE = 64
VDIM = 128
NZ, NX, NC, NY = 8, 4, 2, 4
CAP = 8
ROWS = 256

rope_base = 10000.0
norm_eps = 1e-06


def scale_rows(values, gain_vec):
    as_float = values.astype(jnp.float32)
    factor = lax.rsqrt(jnp.mean(as_float * as_float, axis=-1, keepdims=True) + norm_eps)
    return (as_float * factor * gain_vec.astype(jnp.float32)).astype(jnp.bfloat16)


def rotate(values, positions):
    half_dim = values.shape[-1] // 2
    frequency = rope_base ** (-jnp.arange(half_dim, dtype=jnp.float32) / half_dim)
    angles = positions.astype(jnp.float32)[:, None, None] * frequency
    cosine = jnp.cos(angles)
    sine_part = jnp.sin(angles)
    as_float = values.astype(jnp.float32)
    first_half = as_float[..., :half_dim]
    second_half = as_float[..., half_dim:]
    return jnp.concatenate(
        [
            first_half * cosine - second_half * sine_part,
            first_half * sine_part + second_half * cosine,
        ],
        axis=-1,
    ).astype(jnp.bfloat16)


LOG2E = 1.4426950408889634
MESH_ID = pl.DeviceIdType.MESH
SUBS = 4
WIDE = 512
OFFS = (0, -1, 1, -2, 2, -3, 3, -4)
HALF = 160


def ring(value, size):
    return lax.rem(value + size, size)


def greet(partners):
    barrier = pltpu.get_barrier_semaphore()
    for dev in partners:
        pl.semaphore_signal(barrier, inc=1, device_id=dev, device_id_type=MESH_ID)
    pl.semaphore_wait(barrier, len(partners))


def gather_attend_kernel(
    pay_ref, tab_ref, q_ref, ku_ref, vu_ref, op_ref, res_ref, fg_ref, hid_ref, norm_ref, tabs_ref,
    G, T, m_ref, l_ref, acc_ref, W, HS, HX,
    recv, trecv, zsend, tsend, xsend, fsend, ysend, csend, lsem,
    wrecv, wsend, wfsend, wcsend, hrecv, hsend,
):
    z, x, c, y = (lax.axis_index(n) for n in ("z", "x", "core", "y"))
    hm = lax.rem(y, 2)
    ho = 1 - hm
    up, down = {"z": ring(z + 1, NZ)}, {"z": ring(z - 1, NZ)}
    right, left = {"x": ring(x + 1, NX)}, {"x": ring(x - 1, NX)}
    above, below = {"y": ring(y + 1, NY)}, {"y": ring(y - 1, NY)}
    mate = {"core": 1 - c}
    xs = {0: x, -1: ring(x - 1, NX), 1: ring(x + 1, NX), 2: ring(x + 2, NX)}
    ZZ = [ring(z + off, NZ) for off in OFFS]
    greet([up, down, right, left, above, below, mate])

    def piece(zz, xx, h, sem, dev):
        slot = G.at[c, zz, xx, h]
        return pltpu.make_async_remote_copy(
            src_ref=slot, dst_ref=slot, send_sem=sem, recv_sem=recv.at[c, zz, xx, h],
            device_id=dev, device_id_type=MESH_ID,
        )

    def arrived(par, zz, xx, h):
        slot = G.at[par, zz, xx, h]
        pltpu.make_async_remote_copy(
            src_ref=slot, dst_ref=slot, send_sem=csend, recv_sem=recv.at[par, zz, xx, h],
            device_id=mate, device_id_type=MESH_ID,
        ).wait_recv()

    sent = []

    def send(zz, xx, h, sems, at, dev):
        piece(zz, xx, h, sems.at[at], dev).start()
        sent.append(lambda: piece(zz, xx, h, sems.at[at], dev).wait_send())

    def to_mate(zz, xx, h):
        piece(zz, xx, h, csend, mate).start()

    def table(zz, sem, dev):
        return pltpu.make_async_remote_copy(
            src_ref=T.at[zz], dst_ref=T.at[zz], send_sem=sem, recv_sem=trecv.at[zz],
            device_id=dev, device_id_type=MESH_ID,
        )

    def send_table(zz, at, dev):
        table(zz, tsend.at[at], dev).start()
        sent.append(lambda: table(zz, tsend.at[at], dev).wait_send())

    def ev_z(i):
        off = OFFS[i]
        zz = ZZ[i]
        for h in range(2):
            if i > 0:
                arrived(c, zz, x, h)
            if -4 < off <= 0:
                send(zz, x, h, zsend, (0, -off, h), up)
            if 0 <= off < 3:
                send(zz, x, h, zsend, (1, off, h), down)
            to_mate(zz, x, h)
        send(zz, x, hm, xsend, (i, 0), right)
        send(zz, x, hm, xsend, (i, 1), left)
        if i > 0:
            table(zz, tsend.at[0, 0], up).wait_recv()
        if -4 < off <= 0:
            send_table(zz, (0, -off), up)
        if 0 <= off < 3:
            send_table(zz, (1, off), down)

    def to_y(i, j, zz, xx):
        send(zz, xx, hm, ysend, (i, j), above if (i + j) % 2 == 0 else below)

    def ev_x1(i):
        zz = ZZ[i]
        arrived(c, zz, xs[-1], hm)
        if i % 2 == 0:
            send(zz, xs[-1], hm, fsend, (i,), right)
        to_y(i, 0, zz, xs[-1])
        to_mate(zz, xs[-1], hm)
        arrived(c, zz, xs[1], hm)
        if i % 2 == 1:
            send(zz, xs[1], hm, fsend, (i,), left)
        to_y(i, 1, zz, xs[1])
        to_mate(zz, xs[1], hm)

    def ev_x2(i):
        zz = ZZ[i]
        arrived(c, zz, xs[2], hm)
        to_y(i, 2, zz, xs[2])
        to_mate(zz, xs[2], hm)

    def ev_y(i, dx):
        zz = ZZ[i]
        arrived(c, zz, xs[dx], ho)
        to_mate(zz, xs[dx], ho)

    yb, ya, y2 = ring(y - 1, NY), ring(y + 1, NY), ring(y + 2, NY)

    def proj(yy, r, sem, dev):
        slot = W.at[yy, c, r]
        return pltpu.make_async_remote_copy(
            src_ref=slot, dst_ref=slot, send_sem=sem, recv_sem=wrecv.at[yy, c, r],
            device_id=dev, device_id_type=MESH_ID,
        )

    def proj_in(yy, half, r):
        slot = W.at[yy, half, r]
        pltpu.make_async_remote_copy(
            src_ref=slot, dst_ref=slot, send_sem=wcsend, recv_sem=wrecv.at[yy, half, r],
            device_id=mate, device_id_type=MESH_ID,
        ).wait_recv()

    def proj_send(yy, r, sems, where, dev):
        proj(yy, r, sems.at[where], dev).start()
        sent.append(lambda: proj(yy, r, sems.at[where], dev).wait_send())

    def ev_proj(r):
        proj_send(y, r, wsend, (0, r), above)
        proj_send(y, r, wsend, (1, r), below)

    def ev_proj1(r):
        proj_in(yb, c, r)
        if r % 2 == 0:
            proj_send(yb, r, wfsend, (r,), above)
        proj(yb, r, wcsend, mate).start()
        proj_in(ya, c, r)
        if r % 2 == 1:
            proj_send(ya, r, wfsend, (r,), below)
        proj(ya, r, wcsend, mate).start()

    def ev_proj2(r):
        proj_in(y2, c, r)
        proj(y2, r, wcsend, mate).start()

    own_proj = [
        pltpu.make_async_copy(
            op_ref.at[:, :, half * 1024 : (half + 1) * 1024], W.at[y, half], lsem.at[2 + half]
        )
        for half in range(2)
    ]
    for copy in own_proj:
        copy.start()
    own = pltpu.make_async_copy(pay_ref, G.at[c, z, x], lsem.at[0])
    own_table = pltpu.make_async_copy(tab_ref, T.at[z], lsem.at[1])
    own.start()
    own_table.start()
    own.wait()
    own_table.wait()

    m_ref[...] = jnp.full(m_ref.shape, -1e30, jnp.float32)
    l_ref[...] = jnp.zeros(l_ref.shape, jnp.float32)
    acc_ref[...] = jnp.zeros(acc_ref.shape, jnp.float32)
    scale = LOG2E / math.sqrt(NOPE + ROPE)
    keys = 512

    def compute(zz, xx, masked):
        lat = jnp.concatenate(
            [G[par, zz, xx, h, 0:128, :] for par in range(2) for h in range(2)], axis=0
        )
        rope = jnp.concatenate(
            [
                G[par, zz, xx, h, 128:HALF, g * ROPE : (g + 1) * ROPE]
                for par in range(2)
                for h in range(2)
                for g in range(4)
            ],
            axis=0,
        )
        rope = jnp.concatenate([rope, jnp.zeros((keys, ROPE), jnp.bfloat16)], axis=1)
        k = jnp.dot(lat, ku_ref[...], preferred_element_type=jnp.float32).astype(jnp.bfloat16)
        v = jnp.dot(lat, vu_ref[...], preferred_element_type=jnp.float32).astype(jnp.bfloat16)
        if masked:
            kpos = lax.broadcasted_iota(jnp.int32, (1, keys), 1)
            qpos = c * ROWS + lax.broadcasted_iota(jnp.int32, (ROWS, 1), 0)
            allowed = kpos <= qpos
        for h in range(2):
            kcat = jnp.concatenate([k[:, h * NOPE : (h + 1) * NOPE], rope], axis=1)
            s = lax.dot_general(
                q_ref[h], kcat, (((1,), (1,)), ((), ())), preferred_element_type=jnp.float32
            )
            s = s * scale
            if masked:
                s = jnp.where(allowed, s, -1e30)
            m_old = m_ref[h]
            m_new = jnp.maximum(m_old, jnp.max(s, axis=1, keepdims=True))
            p = jnp.exp2(s - m_new[:, :1])
            if masked:
                p = jnp.where(allowed, p, 0.0)
            alpha = jnp.exp2(m_old - m_new)
            l_ref[h] = l_ref[h] * alpha + jnp.sum(p, axis=1, keepdims=True)
            acc_ref[h] = acc_ref[h] * alpha + jnp.dot(
                p.astype(jnp.bfloat16),
                v[:, h * VDIM : (h + 1) * VDIM],
                preferred_element_type=jnp.float32,
            )
            m_ref[h] = m_new

    mine = z * NX + x

    def round_(s, carry):
        for k in range(11):

            @pl.when(s == k)
            def _():
                if k < 8:
                    ev_z(k)
                if 0 <= k - 1 < 8:
                    ev_x1(k - 1)
                if 0 <= k - 2 < 8:
                    ev_x2(k - 2)
                    ev_y(k - 2, -1)
                    ev_y(k - 2, 1)
                if 0 <= k - 3 < 8:
                    ev_y(k - 3, 2)
                if k == 1:
                    for copy in own_proj:
                        copy.wait()
                if 0 <= k - 1 < 8:
                    ev_proj(k - 1)
                if 0 <= k - 2 < 8:
                    ev_proj1(k - 2)
                if 0 <= k - 3 < 8:
                    ev_proj2(k - 3)

        def pair(d, carry):
            i = s - 1 - jnp.where(d == 0, 0, jnp.where(d == 3, 3, 2))

            @pl.when((i >= 0) & (i < 8))
            def _():
                off = jnp.where(lax.rem(i, 2) == 1, -((i + 1) // 2), i // 2)
                dx = jnp.where(d == 3, 2, jnp.where(d == 1, -1, jnp.where(d == 2, 1, 0)))
                zz = ring(z + off, NZ)
                xx = ring(x + dx, NX)
                for h in range(2):
                    arrived(1 - c, zz, xx, h)
                theirs = zz * NX + xx

                @pl.when(theirs < mine)
                def _():
                    compute(zz, xx, False)

                @pl.when(theirs == mine)
                def _():
                    compute(zz, xx, True)

            return carry

        return lax.fori_loop(0, 4, pair, carry)

    lax.fori_loop(0, 12, round_, 0)

    for h in range(2):
        heads = (acc_ref[h] / l_ref[h]).astype(jnp.bfloat16)
        for q in range(NY):
            HS[q, :, h * VDIM : (h + 1) * VDIM] = heads[q * 64 : (q + 1) * 64]

    def heads_to(yy):
        return pltpu.make_async_remote_copy(
            src_ref=HS.at[yy], dst_ref=HX.at[y], send_sem=hsend.at[yy], recv_sem=hrecv.at[y],
            device_id={"y": yy}, device_id_type=MESH_ID,
        )

    for yy in (y2, ya, yb):
        heads_to(yy).start()
    HX[y] = HS[y]
    tabs_ref[...] = T[...]
    for yy in (yb, ya, y2):
        for r in range(8):
            proj_in(yy, 1 - c, r)
    for yy in (yb, ya, y2):
        pltpu.make_async_remote_copy(
            src_ref=HS.at[yy], dst_ref=HX.at[yy], send_sem=hsend.at[yy], recv_sem=hrecv.at[yy],
            device_id={"y": yy}, device_id_type=MESH_ID,
        ).wait_recv()
    squares = jnp.zeros((64, 1), jnp.float32)
    for half in range(2):
        lanes = slice(half * 1024, (half + 1) * 1024)
        total = jnp.zeros((64, 1024), jnp.float32)
        for q in range(NY):
            weight = jnp.concatenate([W[q, half, r] for r in range(8)], axis=0)
            rows = jnp.dot(HX[q], weight, preferred_element_type=jnp.float32)
            total = total + rows.astype(jnp.bfloat16).astype(jnp.float32)
        one = (res_ref[:, lanes].astype(jnp.float32) + total).astype(jnp.bfloat16)
        hid_ref[:, lanes] = one
        one = one.astype(jnp.float32)
        squares = squares + jnp.sum(one * one, axis=1, keepdims=True)
    factor = lax.rsqrt(squares * (1.0 / 2048) + norm_eps)
    norm_ref[...] = (
        hid_ref[...].astype(jnp.float32) * factor * fg_ref[...].astype(jnp.float32)
    ).astype(jnp.bfloat16)
    for yy in (y2, ya, yb):
        heads_to(yy).wait_send()
    pltpu.make_async_remote_copy(
        src_ref=W.at[0:3, 0], dst_ref=W.at[0:3, 0], send_sem=wcsend, recv_sem=wrecv.at[0, 0, 0],
        device_id=mate, device_id_type=MESH_ID,
    ).wait_send()
    for wait in sent:
        wait()
    whole = G.at[c]
    pltpu.make_async_remote_copy(
        src_ref=whole, dst_ref=whole, send_sem=csend, recv_sem=recv.at[0, 0, 0, 0],
        device_id=mate, device_id_type=MESH_ID,
    ).wait_send()


def gather_attend(payload, tables, q_cat, key_local, value_local, out_proj, residual, gain):
    vmem = pl.BlockSpec(memory_space=pltpu.VMEM)
    hbm = pl.BlockSpec(memory_space=pl.ANY)
    return pl.pallas_call(
        gather_attend_kernel,
        out_shape=(
            jax.ShapeDtypeStruct((64, 2048), jnp.bfloat16),
            jax.ShapeDtypeStruct((64, 2048), jnp.bfloat16),
            jax.ShapeDtypeStruct((NZ, 8, 128), jnp.float32),
        ),
        in_specs=[vmem] * 5 + [hbm, vmem, vmem],
        out_specs=(vmem, vmem, vmem),
        scratch_shapes=[
            pltpu.VMEM((2, NZ, NX, 2, HALF, 256), jnp.bfloat16),
            pltpu.VMEM((NZ, 8, 128), jnp.float32),
            pltpu.VMEM((2, ROWS, 128), jnp.float32),
            pltpu.VMEM((2, ROWS, 128), jnp.float32),
            pltpu.VMEM((2, ROWS, 128), jnp.float32),
            pltpu.VMEM((NY, 2, 8, 32, 1024), jnp.bfloat16),
            pltpu.VMEM((NY, 64, 256), jnp.bfloat16),
            pltpu.VMEM((NY, 64, 256), jnp.bfloat16),
            pltpu.SemaphoreType.DMA((2, NZ, NX, 2)),
            pltpu.SemaphoreType.DMA((NZ,)),
            pltpu.SemaphoreType.DMA((2, 4, 2)),
            pltpu.SemaphoreType.DMA((2, 4)),
            pltpu.SemaphoreType.DMA((8, 2)),
            pltpu.SemaphoreType.DMA((8,)),
            pltpu.SemaphoreType.DMA((8, 3)),
            pltpu.SemaphoreType.DMA,
            pltpu.SemaphoreType.DMA((4,)),
            pltpu.SemaphoreType.DMA((NY, 2, 8)),
            pltpu.SemaphoreType.DMA((2, 8)),
            pltpu.SemaphoreType.DMA((8,)),
            pltpu.SemaphoreType.DMA,
            pltpu.SemaphoreType.DMA((NY,)),
            pltpu.SemaphoreType.DMA((NY,)),
        ],
        compiler_params=pltpu.CompilerParams(
            collective_id=0, has_side_effects=True, vmem_limit_bytes=63 * 1024 * 1024
        ),
    )(
        payload, tables, q_cat, key_local, value_local, out_proj.reshape(8, 32, 2048), residual,
        gain.reshape(1, 2048),
    )


def moe_kernel(
    norm_ref, hid_ref, tab_ref, wg_h, wu_h, wd_h, sg_h, su_h, sd_h, out_ref,
    COL, OUT, ARR, EO, RET, PART, RD, RU, wg, wu, wd, sg, su, sd,
    zrecv, zsend, arecv, asend, rrecv, rsend, drecv, dsend, lsem, wsem,
):
    z, x, c, y = (lax.axis_index(n) for n in ("z", "x", "core", "y"))
    me = x * NC + c
    up, down = {"z": ring(z + 1, NZ)}, {"z": ring(z - 1, NZ)}
    peers = []
    for q in range(1, 8):
        p = ring(me + q, 8)
        peers.append((p, {"x": p // NC, "core": lax.rem(p, NC)}))

    weights = [
        pltpu.make_async_copy(src, dst, wsem.at[n])
        for n, (src, dst) in enumerate(
            ((sg_h, sg), (su_h, su), (sd_h, sd), (wg_h, wg), (wu_h, wu), (wd_h, wd))
        )
    ]
    for b in range(SUBS):
        COL[0, b] = norm_ref[:, b * WIDE : (b + 1) * WIDE]
    for w in weights:
        w.start()
    greet([up, down] + [dev for _, dev in peers])

    at = {off: i for i, off in enumerate(OFFS)}

    def along_z(i, b, dev, off_to, n):
        there = at[off_to]
        return pltpu.make_async_remote_copy(
            src_ref=COL.at[i, b], dst_ref=COL.at[there, b], send_sem=zsend.at[n, b],
            recv_sem=zrecv.at[there, b], device_id=dev, device_id_type=MESH_ID,
        )

    def pass_on(off, b):
        i = at[off]
        if off != 0:
            along_z(i, b, up, off, 0).wait_recv()
        if -3 < off <= 0 or (off == -3 and b < 2):
            start(along_z(i, b, up, off - 1, -off))
        if 0 <= off < 3:
            start(along_z(i, b, down, off + 1, 4 + off))
        if off == 3 and b >= 2:
            start(along_z(i, b, down, -4, 7))

    sends = []

    def start(copy):
        copy.start()
        sends.append(copy)

    def pieces(i, src, dst, sems_send, sems_recv):
        for p, dev in peers:
            pltpu.make_async_remote_copy(
                src_ref=src.at[i, p], dst_ref=dst.at[i, me], send_sem=sems_send.at[i],
                recv_sem=sems_recv.at[i], device_id=dev, device_id_type=MESH_ID,
            ).start()
        pltpu.make_async_copy(src.at[i, me], dst.at[i, me], lsem.at[1]).start()
        pltpu.make_async_copy(src.at[i, me], dst.at[i, me], lsem.at[1]).wait()

    def pieces_in(i, dst, sems_recv):
        ref = dst.at[i, 0:7]
        pltpu.make_async_remote_copy(
            src_ref=ref, dst_ref=ref, send_sem=lsem.at[2], recv_sem=sems_recv.at[i],
            device_id=peers[0][1], device_id_type=MESH_ID,
        ).wait_recv()

    def pieces_sent(i, src, sems_send):
        ref = src.at[i, 0:7]
        pltpu.make_async_remote_copy(
            src_ref=ref, dst_ref=ref, send_sem=sems_send.at[i], recv_sem=lsem.at[2],
            device_id=peers[0][1], device_id_type=MESH_ID,
        ).wait_send()

    slots = lax.broadcasted_iota(jnp.int32, (64, 64), 0).astype(jnp.float32)

    def matches(i):
        tab = tab_ref[ring(z + OFFS[i], NZ)]
        base = (z * 64).astype(jnp.float32)
        return [(tab[k : k + 1, 0:64] - base) == slots for k in range(4)], tab

    def picks(i):
        hit, _ = matches(i)
        return jnp.where(hit[0] | hit[1] | hit[2] | hit[3], 1.0, 0.0).astype(jnp.bfloat16)

    def select(i, b, pick):
        rows = jnp.dot(pick, COL[i, b], preferred_element_type=jnp.float32)
        for p in range(8):
            OUT[i, p, :, b * WIDE : (b + 1) * WIDE] = rows[p * CAP : (p + 1) * CAP].astype(
                jnp.bfloat16
            )

    def gated(rows, gate, upper, lower):
        g = jnp.dot(rows, gate[...], preferred_element_type=jnp.float32)
        u = jnp.dot(rows, upper[...], preferred_element_type=jnp.float32)
        hidden = (g / (1.0 + jnp.exp(-g)) * u).astype(jnp.bfloat16)
        return jnp.dot(hidden, lower[...], preferred_element_type=jnp.float32)

    def expert(group):
        for i in group:
            pieces_in(i, ARR, arecv)
        rows = jnp.concatenate(
            [ARR[i, p].astype(jnp.float32) for i in group for p in range(8)], axis=0
        ).astype(jnp.bfloat16)
        done = gated(rows, wg, wu, wd)
        for n, i in enumerate(group):
            for p in range(8):
                lo = (n * 8 + p) * CAP
                EO[i, p] = done[lo : lo + CAP].astype(jnp.bfloat16)
            pieces(i, EO, RET, rsend, rrecv)

    def combine(i):
        pieces_in(i, RET, rrecv)
        hit, tab = matches(i)
        share = jnp.zeros((64, 64), jnp.float32)
        for k in range(4):
            share = share + jnp.where(hit[k], tab[4 + k : 5 + k, 0:64], 0.0)
        hi = share.astype(jnp.bfloat16)
        lo = (share - hi.astype(jnp.float32)).astype(jnp.bfloat16)
        back = jnp.concatenate(
            [RET[i, p].astype(jnp.float32) for p in range(8)], axis=0
        ).astype(jnp.bfloat16)
        dims = (((0,), (0,)), ((), ()))
        total = lax.dot_general(hi, back, dims, preferred_element_type=jnp.float32)
        total = total + lax.dot_general(lo, back, dims, preferred_element_type=jnp.float32)
        for b in range(SUBS):
            PART[i, b] = total[:, b * WIDE : (b + 1) * WIDE].astype(jnp.bfloat16)

    groups = ((0,), (1, 2), (3, 4), (5, 6), (7,))

    def shared():
        for w in weights[:3]:
            w.wait()
        rows = jnp.concatenate([COL[0, b] for b in range(SUBS)], axis=1)
        out_ref[...] = (
            hid_ref[...].astype(jnp.float32)
            + gated(rows, sg, su, sd).astype(jnp.bfloat16).astype(jnp.float32)
        )

    def between(s, b):
        if s == 1 and b == 3:
            shared()
        if s >= 2 and b == 1:
            if s == 2:
                for w in weights[3:]:
                    w.wait()
            expert(groups[s - 2])
        if s >= 3 and b >= 2 and b - 2 < len(groups[s - 3]):
            combine(groups[s - 3][b - 2])

    for s in range(5):
        pick = [picks(i) for i in groups[s]]
        for b in range(SUBS):
            for n, i in enumerate(groups[s]):
                pass_on(OFFS[i], b)
            for n, i in enumerate(groups[s]):
                select(i, b, pick[n])
            between(s, b)
        for i in groups[s]:
            pieces(i, OUT, ARR, asend, arecv)
    expert(groups[3])
    for i in groups[2]:
        combine(i)
    expert(groups[4])

    def back_z(i, b, way, k):
        dst, dev = ((RD, down), (RU, up))[way]
        return pltpu.make_async_remote_copy(
            src_ref=PART.at[i, b], dst_ref=dst.at[k, b], send_sem=dsend.at[way, k, b],
            recv_sem=drecv.at[way, k, b], device_id=dev, device_id_type=MESH_ID,
        )

    def chain(way, k, b):
        i = at[-k if way == 0 or k == 4 else k]
        if k < 3 or (k == 3 and (b < 2) == (way == 0)):
            back_z(i, b, way, k).wait_recv()
            dst = (RD, RU)[way]
            PART[i, b] = (
                PART[i, b].astype(jnp.float32) + dst[k, b].astype(jnp.float32)
            ).astype(jnp.bfloat16)
        start(back_z(i, b, way, k - 1))

    combine(groups[3][0])
    for b in (2, 3):
        chain(0, 3, b)
    combine(groups[3][1])
    for b in (0, 1):
        chain(1, 3, b)
    combine(groups[4][0])
    for n in range(2):
        chain(0, 4, n)
        chain(1, 4, n + 2)
    for k in (3, 2, 1):
        for n in range(4):
            down_b, up_b = (n + 2) % 4, n
            if k < 3 or down_b < 2:
                chain(0, k, down_b)
            if k < 3 or up_b >= 2:
                chain(1, k, up_b)
    for n in range(4):
        back_z(0, n, 0, 0).wait_recv()
        back_z(0, n, 1, 0).wait_recv()
        lanes = slice(n * WIDE, (n + 1) * WIDE)
        routed = (
            PART[0, n].astype(jnp.float32)
            + RD[0, n].astype(jnp.float32)
            + RU[0, n].astype(jnp.float32)
        )
        out_ref[:, lanes] = out_ref[:, lanes] + routed.astype(jnp.bfloat16).astype(jnp.float32)

    for copy in sends:
        copy.wait_send()
    for i in range(8):
        pieces_sent(i, OUT, asend)
        pieces_sent(i, EO, rsend)


def experts_layer(normed, hidden, tables, wg, wu, wd, sg, su, sd):
    vmem = pl.BlockSpec(memory_space=pltpu.VMEM)
    hbm = pl.BlockSpec(memory_space=pl.ANY)
    d, f = wg.shape
    bf = jnp.bfloat16
    return pl.pallas_call(
        moe_kernel,
        out_shape=jax.ShapeDtypeStruct((64, d), jnp.float32),
        in_specs=[vmem] * 3 + [hbm] * 6,
        out_specs=vmem,
        scratch_shapes=[
            pltpu.VMEM((8, SUBS, 64, WIDE), bf),
            pltpu.VMEM((8, 8, CAP, d), bf),
            pltpu.VMEM((8, 8, CAP, d), bf),
            pltpu.VMEM((8, 8, CAP, d), bf),
            pltpu.VMEM((8, 8, CAP, d), bf),
            pltpu.VMEM((8, SUBS, 64, WIDE), bf),
            pltpu.VMEM((4, SUBS, 64, WIDE), bf),
            pltpu.VMEM((4, SUBS, 64, WIDE), bf),
            pltpu.VMEM((d, f), bf),
            pltpu.VMEM((d, f), bf),
            pltpu.VMEM((f, d), bf),
            pltpu.VMEM((d, f), bf),
            pltpu.VMEM((d, f), bf),
            pltpu.VMEM((f, d), bf),
            pltpu.SemaphoreType.DMA((8, SUBS)),
            pltpu.SemaphoreType.DMA((8, SUBS)),
            pltpu.SemaphoreType.DMA((8,)),
            pltpu.SemaphoreType.DMA((8,)),
            pltpu.SemaphoreType.DMA((8,)),
            pltpu.SemaphoreType.DMA((8,)),
            pltpu.SemaphoreType.DMA((2, 4, SUBS)),
            pltpu.SemaphoreType.DMA((2, 4, SUBS)),
            pltpu.SemaphoreType.DMA((3,)),
            pltpu.SemaphoreType.DMA((6,)),
        ],
        compiler_params=pltpu.CompilerParams(
            collective_id=1, has_side_effects=True, vmem_limit_bytes=63 * 1024 * 1024
        ),
    )(normed, hidden, tables, wg, wu, wd, sg, su, sd)


def body(
    query_nope,
    query_rope,
    latent,
    key_rope,
    latent_gain,
    key_up,
    value_up,
    out_proj,
    residual,
    ffn_gain,
    expert_ids,
    route_weights,
    expert_gate,
    expert_up,
    expert_down,
    shared_gate,
    shared_up,
    shared_down,
):
    z, x, core, y = (lax.axis_index(n) for n in ("z", "x", "core", "y"))
    q_sp = (z * NX + x) * NC + core
    first_row = q_sp * ROWS
    positions = first_row + jnp.arange(ROWS, dtype=jnp.int32)

    normed_latent = scale_rows(latent, latent_gain)
    rot_key = rotate(key_rope[:, None, :], positions)[:, 0, :]
    packed = rot_key.reshape(2, 4, 32, ROPE).transpose(0, 2, 1, 3).reshape(2, 32, 256)
    payload = jnp.concatenate([normed_latent.reshape(2, 128, 256), packed], axis=1)

    key_local = lax.dynamic_slice_in_dim(key_up, y * 256, 256, 1)
    value_local = lax.dynamic_slice_in_dim(value_up, y * 256, 256, 1)
    rot_query = rotate(query_rope.reshape(ROWS, 2, ROPE), positions)
    q_cat = jnp.concatenate(
        [
            query_nope.reshape(ROWS, 2, NOPE),
            rot_query,
            jnp.zeros((ROWS, 2, 64), jnp.bfloat16),
        ],
        axis=-1,
    ).transpose(1, 0, 2)

    flat_ids = expert_ids.reshape(-1)
    onehot = (flat_ids[:, None] == jnp.arange(64, dtype=jnp.int32)[None, :]).astype(jnp.float32)
    earlier = (
        jnp.arange(256, dtype=jnp.int32)[None, :] < jnp.arange(256, dtype=jnp.int32)[:, None]
    ).astype(jnp.float32)
    before = jnp.dot(earlier, onehot)
    rank = jnp.sum(before * onehot, axis=1).reshape(64, 4)
    tables = jnp.concatenate([expert_ids.astype(jnp.float32) * CAP + rank, route_weights], axis=1)
    tables = jnp.concatenate([tables.T, jnp.zeros((8, 64), jnp.float32)], axis=1)
    hidden_one, normed, gathered = gather_attend(
        payload, tables, q_cat, key_local, value_local, out_proj, residual, ffn_gain
    )
    summed = experts_layer(
        normed, hidden_one, gathered, expert_gate[0], expert_up[0], expert_down[0],
        shared_gate, shared_up, shared_down,
    )
    return summed.astype(jnp.bfloat16)


def solution(mesh):
    fine = Mesh(mesh.devices.reshape(NZ, NX, NC, NY), ("z", "x", "core", "y"))
    sp = ("z", "x", "core")
    every = ("z", "x", "core", "y")
    in_specs = (
        P(sp, "y"),
        P(sp, "y"),
        P(sp, None),
        P(sp, None),
        P(),
        P(),
        P(),
        P("y", None),
        P(every, None),
        P(),
        P(every, None),
        P(every, None),
        P(sp, None, None),
        P(sp, None, None),
        P(sp, None, None),
        P(),
        P(),
        P(),
    )
    return jax.shard_map(
        body, mesh=fine, in_specs=in_specs, out_specs=P(every, None), check_vma=False
    )
```

```python
import math

import jax
import jax.numpy as jnp
from jax import lax
from jax.experimental import pallas as pl
from jax.experimental.pallas import tpu as pltpu
from jax.sharding import Mesh, PartitionSpec as P

NOPE = 128
ROPE = 64
VDIM = 128
NZ, NX, NC, NY = 8, 4, 2, 4
CAP = 8
ROWS = 256

rope_base = 10000.0
norm_eps = 1e-06


def scale_rows(values, gain_vec):
    as_float = values.astype(jnp.float32)
    factor = lax.rsqrt(jnp.mean(as_float * as_float, axis=-1, keepdims=True) + norm_eps)
    return (as_float * factor * gain_vec.astype(jnp.float32)).astype(jnp.bfloat16)


def rotate(values, positions):
    half_dim = values.shape[-1] // 2
    frequency = rope_base ** (-jnp.arange(half_dim, dtype=jnp.float32) / half_dim)
    angles = positions.astype(jnp.float32)[:, None, None] * frequency
    cosine = jnp.cos(angles)
    sine_part = jnp.sin(angles)
    as_float = values.astype(jnp.float32)
    first_half = as_float[..., :half_dim]
    second_half = as_float[..., half_dim:]
    return jnp.concatenate(
        [
            first_half * cosine - second_half * sine_part,
            first_half * sine_part + second_half * cosine,
        ],
        axis=-1,
    ).astype(jnp.bfloat16)


LOG2E = 1.4426950408889634
MESH_ID = pl.DeviceIdType.MESH
SUBS = 4
WIDE = 512
OFFS = (0, -1, 1, -2, 2, -3, 3, -4)
HALF = 160


def ring(value, size):
    return lax.rem(value + size, size)


def greet(partners):
    barrier = pltpu.get_barrier_semaphore()
    for dev in partners:
        pl.semaphore_signal(barrier, inc=1, device_id=dev, device_id_type=MESH_ID)
    pl.semaphore_wait(barrier, len(partners))


def gather_attend_kernel(
    pay_ref, tab_ref, q_ref, ku_ref, vu_ref, op_ref, res_ref, fg_ref, hid_ref, norm_ref, tabs_ref,
    G, T, m_ref, l_ref, acc_ref, W, HS, HX,
    recv, trecv, zsend, tsend, xsend, fsend, ysend, csend, lsem,
    wrecv, wsend, wfsend, wcsend, hrecv, hsend,
):
    z, x, c, y = (lax.axis_index(n) for n in ("z", "x", "core", "y"))
    hm = lax.rem(y, 2)
    ho = 1 - hm
    up, down = {"z": ring(z + 1, NZ)}, {"z": ring(z - 1, NZ)}
    right, left = {"x": ring(x + 1, NX)}, {"x": ring(x - 1, NX)}
    above, below = {"y": ring(y + 1, NY)}, {"y": ring(y - 1, NY)}
    mate = {"core": 1 - c}
    xs = {0: x, -1: ring(x - 1, NX), 1: ring(x + 1, NX), 2: ring(x + 2, NX)}
    ZZ = [ring(z + off, NZ) for off in OFFS]
    greet([up, down, right, left, above, below, mate])

    def piece(zz, xx, h, sem, dev):
        slot = G.at[c, zz, xx, h]
        return pltpu.make_async_remote_copy(
            src_ref=slot, dst_ref=slot, send_sem=sem, recv_sem=recv.at[c, zz, xx, h],
            device_id=dev, device_id_type=MESH_ID,
        )

    def arrived(par, zz, xx, h):
        slot = G.at[par, zz, xx, h]
        pltpu.make_async_remote_copy(
            src_ref=slot, dst_ref=slot, send_sem=csend, recv_sem=recv.at[par, zz, xx, h],
            device_id=mate, device_id_type=MESH_ID,
        ).wait_recv()

    sent = []

    def send(zz, xx, h, sems, at, dev):
        piece(zz, xx, h, sems.at[at], dev).start()
        sent.append(lambda: piece(zz, xx, h, sems.at[at], dev).wait_send())

    def to_mate(zz, xx, h):
        piece(zz, xx, h, csend, mate).start()

    def table(zz, sem, dev):
        return pltpu.make_async_remote_copy(
            src_ref=T.at[zz], dst_ref=T.at[zz], send_sem=sem, recv_sem=trecv.at[zz],
            device_id=dev, device_id_type=MESH_ID,
        )

    def send_table(zz, at, dev):
        table(zz, tsend.at[at], dev).start()
        sent.append(lambda: table(zz, tsend.at[at], dev).wait_send())

    def ev_z(i):
        off = OFFS[i]
        zz = ZZ[i]
        for h in range(2):
            if i > 0:
                arrived(c, zz, x, h)
            if -4 < off <= 0:
                send(zz, x, h, zsend, (0, -off, h), up)
            if 0 <= off < 3:
                send(zz, x, h, zsend, (1, off, h), down)
            to_mate(zz, x, h)
        send(zz, x, hm, xsend, (i, 0), right)
        send(zz, x, hm, xsend, (i, 1), left)
        if i > 0:
            table(zz, tsend.at[0, 0], up).wait_recv()
        if -4 < off <= 0:
            send_table(zz, (0, -off), up)
        if 0 <= off < 3:
            send_table(zz, (1, off), down)

    def to_y(i, j, zz, xx):
        send(zz, xx, hm, ysend, (i, j), above if (i + j) % 2 == 0 else below)

    def ev_x1(i):
        zz = ZZ[i]
        arrived(c, zz, xs[-1], hm)
        if i % 2 == 0:
            send(zz, xs[-1], hm, fsend, (i,), right)
        to_y(i, 0, zz, xs[-1])
        to_mate(zz, xs[-1], hm)
        arrived(c, zz, xs[1], hm)
        if i % 2 == 1:
            send(zz, xs[1], hm, fsend, (i,), left)
        to_y(i, 1, zz, xs[1])
        to_mate(zz, xs[1], hm)

    def ev_x2(i):
        zz = ZZ[i]
        arrived(c, zz, xs[2], hm)
        to_y(i, 2, zz, xs[2])
        to_mate(zz, xs[2], hm)

    def ev_y(i, dx):
        zz = ZZ[i]
        arrived(c, zz, xs[dx], ho)
        to_mate(zz, xs[dx], ho)

    yb, ya, y2 = ring(y - 1, NY), ring(y + 1, NY), ring(y + 2, NY)

    def proj(yy, r, sem, dev):
        slot = W.at[yy, c, r]
        return pltpu.make_async_remote_copy(
            src_ref=slot, dst_ref=slot, send_sem=sem, recv_sem=wrecv.at[yy, c, r],
            device_id=dev, device_id_type=MESH_ID,
        )

    def proj_in(yy, half, r):
        slot = W.at[yy, half, r]
        pltpu.make_async_remote_copy(
            src_ref=slot, dst_ref=slot, send_sem=wcsend, recv_sem=wrecv.at[yy, half, r],
            device_id=mate, device_id_type=MESH_ID,
        ).wait_recv()

    def proj_send(yy, r, sems, where, dev):
        proj(yy, r, sems.at[where], dev).start()
        sent.append(lambda: proj(yy, r, sems.at[where], dev).wait_send())

    def ev_proj(r):
        proj_send(y, r, wsend, (0, r), above)
        proj_send(y, r, wsend, (1, r), below)

    def ev_proj1(r):
        proj_in(yb, c, r)
        if r % 2 == 0:
            proj_send(yb, r, wfsend, (r,), above)
        proj(yb, r, wcsend, mate).start()
        proj_in(ya, c, r)
        if r % 2 == 1:
            proj_send(ya, r, wfsend, (r,), below)
        proj(ya, r, wcsend, mate).start()

    def ev_proj2(r):
        proj_in(y2, c, r)
        proj(y2, r, wcsend, mate).start()

    own_proj = [
        pltpu.make_async_copy(
            op_ref.at[:, :, half * 1024 : (half + 1) * 1024], W.at[y, half], lsem.at[2 + half]
        )
        for half in range(2)
    ]
    for copy in own_proj:
        copy.start()
    own = pltpu.make_async_copy(pay_ref, G.at[c, z, x], lsem.at[0])
    own_table = pltpu.make_async_copy(tab_ref, T.at[z], lsem.at[1])
    own.start()
    own_table.start()
    own.wait()
    own_table.wait()

    m_ref[...] = jnp.full(m_ref.shape, -1e30, jnp.float32)
    l_ref[...] = jnp.zeros(l_ref.shape, jnp.float32)
    acc_ref[...] = jnp.zeros(acc_ref.shape, jnp.float32)
    scale = LOG2E / math.sqrt(NOPE + ROPE)
    keys = 512

    def compute(zz, xx, masked):
        lat = jnp.concatenate(
            [G[par, zz, xx, h, 0:128, :] for par in range(2) for h in range(2)], axis=0
        )
        rope = jnp.concatenate(
            [
                G[par, zz, xx, h, 128:HALF, g * ROPE : (g + 1) * ROPE]
                for par in range(2)
                for h in range(2)
                for g in range(4)
            ],
            axis=0,
        )
        rope = jnp.concatenate([rope, jnp.zeros((keys, ROPE), jnp.bfloat16)], axis=1)
        k = jnp.dot(lat, ku_ref[...], preferred_element_type=jnp.float32).astype(jnp.bfloat16)
        v = jnp.dot(lat, vu_ref[...], preferred_element_type=jnp.float32).astype(jnp.bfloat16)
        if masked:
            kpos = lax.broadcasted_iota(jnp.int32, (1, keys), 1)
            qpos = c * ROWS + lax.broadcasted_iota(jnp.int32, (ROWS, 1), 0)
            allowed = kpos <= qpos
        for h in range(2):
            kcat = jnp.concatenate([k[:, h * NOPE : (h + 1) * NOPE], rope], axis=1)
            s = lax.dot_general(
                q_ref[h], kcat, (((1,), (1,)), ((), ())), preferred_element_type=jnp.float32
            )
            s = s * scale
            if masked:
                s = jnp.where(allowed, s, -1e30)
            m_old = m_ref[h]
            m_new = jnp.maximum(m_old, jnp.max(s, axis=1, keepdims=True))
            p = jnp.exp2(s - m_new[:, :1])
            if masked:
                p = jnp.where(allowed, p, 0.0)
            alpha = jnp.exp2(m_old - m_new)
            l_ref[h] = l_ref[h] * alpha + jnp.sum(p, axis=1, keepdims=True)
            acc_ref[h] = acc_ref[h] * alpha + jnp.dot(
                p.astype(jnp.bfloat16),
                v[:, h * VDIM : (h + 1) * VDIM],
                preferred_element_type=jnp.float32,
            )
            m_ref[h] = m_new

    mine = z * NX + x

    def round_(s, carry):
        for k in range(13):

            @pl.when(s == k)
            def _():
                if k < 8:
                    ev_z(k)
                if 0 <= k - 1 < 8:
                    ev_x1(k - 1)
                if 0 <= k - 2 < 8:
                    ev_x2(k - 2)
                if 0 <= k - 3 < 8:
                    ev_y(k - 3, -1)
                    ev_y(k - 3, 1)
                if 0 <= k - 4 < 8:
                    ev_y(k - 4, 2)
                if k == 1:
                    for copy in own_proj:
                        copy.wait()
                if 0 <= k - 1 < 8:
                    ev_proj(k - 1)
                if 0 <= k - 3 < 8:
                    ev_proj1(k - 3)
                if 0 <= k - 5 < 8:
                    ev_proj2(k - 5)

        def pair(d, carry):
            i = s - 1 - jnp.where(d == 0, 0, jnp.where(d == 3, 4, 3))

            @pl.when((i >= 0) & (i < 8))
            def _():
                off = jnp.where(lax.rem(i, 2) == 1, -((i + 1) // 2), i // 2)
                dx = jnp.where(d == 3, 2, jnp.where(d == 1, -1, jnp.where(d == 2, 1, 0)))
                zz = ring(z + off, NZ)
                xx = ring(x + dx, NX)
                for h in range(2):
                    arrived(1 - c, zz, xx, h)
                theirs = zz * NX + xx

                @pl.when(theirs < mine)
                def _():
                    compute(zz, xx, False)

                @pl.when(theirs == mine)
                def _():
                    compute(zz, xx, True)

            return carry

        return lax.fori_loop(0, 4, pair, carry)

    lax.fori_loop(0, 13, round_, 0)

    for h in range(2):
        heads = (acc_ref[h] / l_ref[h]).astype(jnp.bfloat16)
        for q in range(NY):
            HS[q, :, h * VDIM : (h + 1) * VDIM] = heads[q * 64 : (q + 1) * 64]

    def heads_to(yy):
        return pltpu.make_async_remote_copy(
            src_ref=HS.at[yy], dst_ref=HX.at[y], send_sem=hsend.at[yy], recv_sem=hrecv.at[y],
            device_id={"y": yy}, device_id_type=MESH_ID,
        )

    for yy in (y2, ya, yb):
        heads_to(yy).start()
    HX[y] = HS[y]
    tabs_ref[...] = T[...]
    for yy in (yb, ya, y2):
        for r in range(8):
            proj_in(yy, 1 - c, r)
    for yy in (yb, ya, y2):
        pltpu.make_async_remote_copy(
            src_ref=HS.at[yy], dst_ref=HX.at[yy], send_sem=hsend.at[yy], recv_sem=hrecv.at[yy],
            device_id={"y": yy}, device_id_type=MESH_ID,
        ).wait_recv()
    squares = jnp.zeros((64, 1), jnp.float32)
    for half in range(2):
        lanes = slice(half * 1024, (half + 1) * 1024)
        total = jnp.zeros((64, 1024), jnp.float32)
        for q in range(NY):
            weight = jnp.concatenate([W[q, half, r] for r in range(8)], axis=0)
            rows = jnp.dot(HX[q], weight, preferred_element_type=jnp.float32)
            total = total + rows.astype(jnp.bfloat16).astype(jnp.float32)
        one = (res_ref[:, lanes].astype(jnp.float32) + total).astype(jnp.bfloat16)
        hid_ref[:, lanes] = one
        one = one.astype(jnp.float32)
        squares = squares + jnp.sum(one * one, axis=1, keepdims=True)
    factor = lax.rsqrt(squares * (1.0 / 2048) + norm_eps)
    norm_ref[...] = (
        hid_ref[...].astype(jnp.float32) * factor * fg_ref[...].astype(jnp.float32)
    ).astype(jnp.bfloat16)
    for yy in (y2, ya, yb):
        heads_to(yy).wait_send()
    pltpu.make_async_remote_copy(
        src_ref=W.at[0:3, 0], dst_ref=W.at[0:3, 0], send_sem=wcsend, recv_sem=wrecv.at[0, 0, 0],
        device_id=mate, device_id_type=MESH_ID,
    ).wait_send()
    for wait in sent:
        wait()
    whole = G.at[c]
    pltpu.make_async_remote_copy(
        src_ref=whole, dst_ref=whole, send_sem=csend, recv_sem=recv.at[0, 0, 0, 0],
        device_id=mate, device_id_type=MESH_ID,
    ).wait_send()


def gather_attend(payload, tables, q_cat, key_local, value_local, out_proj, residual, gain):
    vmem = pl.BlockSpec(memory_space=pltpu.VMEM)
    hbm = pl.BlockSpec(memory_space=pl.ANY)
    return pl.pallas_call(
        gather_attend_kernel,
        out_shape=(
            jax.ShapeDtypeStruct((64, 2048), jnp.bfloat16),
            jax.ShapeDtypeStruct((64, 2048), jnp.bfloat16),
            jax.ShapeDtypeStruct((NZ, 8, 128), jnp.float32),
        ),
        in_specs=[vmem] * 5 + [hbm, vmem, vmem],
        out_specs=(vmem, vmem, vmem),
        scratch_shapes=[
            pltpu.VMEM((2, NZ, NX, 2, HALF, 256), jnp.bfloat16),
            pltpu.VMEM((NZ, 8, 128), jnp.float32),
            pltpu.VMEM((2, ROWS, 128), jnp.float32),
            pltpu.VMEM((2, ROWS, 128), jnp.float32),
            pltpu.VMEM((2, ROWS, 128), jnp.float32),
            pltpu.VMEM((NY, 2, 8, 32, 1024), jnp.bfloat16),
            pltpu.VMEM((NY, 64, 256), jnp.bfloat16),
            pltpu.VMEM((NY, 64, 256), jnp.bfloat16),
            pltpu.SemaphoreType.DMA((2, NZ, NX, 2)),
            pltpu.SemaphoreType.DMA((NZ,)),
            pltpu.SemaphoreType.DMA((2, 4, 2)),
            pltpu.SemaphoreType.DMA((2, 4)),
            pltpu.SemaphoreType.DMA((8, 2)),
            pltpu.SemaphoreType.DMA((8,)),
            pltpu.SemaphoreType.DMA((8, 3)),
            pltpu.SemaphoreType.DMA,
            pltpu.SemaphoreType.DMA((4,)),
            pltpu.SemaphoreType.DMA((NY, 2, 8)),
            pltpu.SemaphoreType.DMA((2, 8)),
            pltpu.SemaphoreType.DMA((8,)),
            pltpu.SemaphoreType.DMA,
            pltpu.SemaphoreType.DMA((NY,)),
            pltpu.SemaphoreType.DMA((NY,)),
        ],
        compiler_params=pltpu.CompilerParams(
            collective_id=0, has_side_effects=True, vmem_limit_bytes=63 * 1024 * 1024
        ),
    )(
        payload, tables, q_cat, key_local, value_local, out_proj.reshape(8, 32, 2048), residual,
        gain.reshape(1, 2048),
    )


def moe_kernel(
    norm_ref, hid_ref, tab_ref, wg_h, wu_h, wd_h, sg_h, su_h, sd_h, out_ref,
    COL, OUT, ARR, EO, RET, PART, RD, RU, wg, wu, wd, sg, su, sd,
    zrecv, zsend, arecv, asend, rrecv, rsend, drecv, dsend, lsem, wsem,
):
    z, x, c, y = (lax.axis_index(n) for n in ("z", "x", "core", "y"))
    me = x * NC + c
    up, down = {"z": ring(z + 1, NZ)}, {"z": ring(z - 1, NZ)}
    peers = []
    for q in range(1, 8):
        p = ring(me + q, 8)
        peers.append((p, {"x": p // NC, "core": lax.rem(p, NC)}))

    weights = [
        pltpu.make_async_copy(src, dst, wsem.at[n])
        for n, (src, dst) in enumerate(
            ((wg_h, wg), (wu_h, wu), (wd_h, wd), (sg_h, sg), (su_h, su), (sd_h, sd))
        )
    ]
    for b in range(SUBS):
        COL[0, b] = norm_ref[:, b * WIDE : (b + 1) * WIDE]
    for w in weights:
        w.start()
    greet([up, down] + [dev for _, dev in peers])

    at = {off: i for i, off in enumerate(OFFS)}

    def along_z(i, b, dev, off_to, n):
        there = at[off_to]
        return pltpu.make_async_remote_copy(
            src_ref=COL.at[i, b], dst_ref=COL.at[there, b], send_sem=zsend.at[n, b],
            recv_sem=zrecv.at[there, b], device_id=dev, device_id_type=MESH_ID,
        )

    def pass_on(off, b):
        i = at[off]
        if off != 0:
            along_z(i, b, up, off, 0).wait_recv()
        if -3 < off <= 0 or (off == -3 and b < 2):
            start(along_z(i, b, up, off - 1, -off))
        if 0 <= off < 3:
            start(along_z(i, b, down, off + 1, 4 + off))
        if off == 3 and b >= 2:
            start(along_z(i, b, down, -4, 7))

    sends = []

    def start(copy):
        copy.start()
        sends.append(copy)

    def pieces(i, src, dst, sems_send, sems_recv):
        for p, dev in peers:
            pltpu.make_async_remote_copy(
                src_ref=src.at[i, p], dst_ref=dst.at[i, me], send_sem=sems_send.at[i],
                recv_sem=sems_recv.at[i], device_id=dev, device_id_type=MESH_ID,
            ).start()
        pltpu.make_async_copy(src.at[i, me], dst.at[i, me], lsem.at[1]).start()
        pltpu.make_async_copy(src.at[i, me], dst.at[i, me], lsem.at[1]).wait()

    def pieces_in(i, dst, sems_recv):
        ref = dst.at[i, 0:7]
        pltpu.make_async_remote_copy(
            src_ref=ref, dst_ref=ref, send_sem=lsem.at[2], recv_sem=sems_recv.at[i],
            device_id=peers[0][1], device_id_type=MESH_ID,
        ).wait_recv()

    def pieces_sent(i, src, sems_send):
        ref = src.at[i, 0:7]
        pltpu.make_async_remote_copy(
            src_ref=ref, dst_ref=ref, send_sem=sems_send.at[i], recv_sem=lsem.at[2],
            device_id=peers[0][1], device_id_type=MESH_ID,
        ).wait_send()

    slots = lax.broadcasted_iota(jnp.int32, (64, 64), 0).astype(jnp.float32)

    def matches(i):
        tab = tab_ref[ring(z + OFFS[i], NZ)]
        base = (z * 64).astype(jnp.float32)
        return [(tab[k : k + 1, 0:64] - base) == slots for k in range(4)], tab

    def picks(i):
        hit, _ = matches(i)
        return jnp.where(hit[0] | hit[1] | hit[2] | hit[3], 1.0, 0.0).astype(jnp.bfloat16)

    def select(i, b, pick):
        rows = jnp.dot(pick, COL[i, b], preferred_element_type=jnp.float32)
        for p in range(8):
            OUT[i, p, :, b * WIDE : (b + 1) * WIDE] = rows[p * CAP : (p + 1) * CAP].astype(
                jnp.bfloat16
            )

    def gated(rows, gate, upper, lower):
        g = jnp.dot(rows, gate[...], preferred_element_type=jnp.float32)
        u = jnp.dot(rows, upper[...], preferred_element_type=jnp.float32)
        hidden = (g / (1.0 + jnp.exp(-g)) * u).astype(jnp.bfloat16)
        return jnp.dot(hidden, lower[...], preferred_element_type=jnp.float32)

    def expert(group):
        for i in group:
            pieces_in(i, ARR, arecv)
        rows = jnp.concatenate(
            [ARR[i, p].astype(jnp.float32) for i in group for p in range(8)], axis=0
        ).astype(jnp.bfloat16)
        done = gated(rows, wg, wu, wd)
        for n, i in enumerate(group):
            for p in range(8):
                lo = (n * 8 + p) * CAP
                EO[i, p] = done[lo : lo + CAP].astype(jnp.bfloat16)

    def combine(i):
        pieces_in(i, RET, rrecv)
        hit, tab = matches(i)
        share = jnp.zeros((64, 64), jnp.float32)
        for k in range(4):
            share = share + jnp.where(hit[k], tab[4 + k : 5 + k, 0:64], 0.0)
        hi = share.astype(jnp.bfloat16)
        lo = (share - hi.astype(jnp.float32)).astype(jnp.bfloat16)
        back = jnp.concatenate(
            [RET[i, p].astype(jnp.float32) for p in range(8)], axis=0
        ).astype(jnp.bfloat16)
        dims = (((0,), (0,)), ((), ()))
        total = lax.dot_general(hi, back, dims, preferred_element_type=jnp.float32)
        total = total + lax.dot_general(lo, back, dims, preferred_element_type=jnp.float32)
        for b in range(SUBS):
            PART[i, b] = total[:, b * WIDE : (b + 1) * WIDE].astype(jnp.bfloat16)

    groups = ((0,), (1, 2), (3, 4), (5, 6), (7,))

    def shared():
        for w in weights[3:]:
            w.wait()
        rows = jnp.concatenate([COL[0, b] for b in range(SUBS)], axis=1)
        out_ref[...] = (
            hid_ref[...].astype(jnp.float32)
            + gated(rows, sg, su, sd).astype(jnp.bfloat16).astype(jnp.float32)
        )

    def between(s, b):
        if s >= 2 and b == 1:
            if s == 2:
                for w in weights[:3]:
                    w.wait()
            expert(groups[s - 2])

    for s in range(5):
        pick = [picks(i) for i in groups[s]]
        for b in range(SUBS):
            for n, i in enumerate(groups[s]):
                pass_on(OFFS[i], b)
            for n, i in enumerate(groups[s]):
                select(i, b, pick[n])
            between(s, b)
        for i in groups[s]:
            pieces(i, OUT, ARR, asend, arecv)
    expert(groups[3])
    expert(groups[4])
    for group in reversed(groups):
        for i in group:
            pieces(i, EO, RET, rsend, rrecv)
    shared()

    def back_z(i, b, way, k):
        dst, dev = ((RD, down), (RU, up))[way]
        return pltpu.make_async_remote_copy(
            src_ref=PART.at[i, b], dst_ref=dst.at[k, b], send_sem=dsend.at[way, k, b],
            recv_sem=drecv.at[way, k, b], device_id=dev, device_id_type=MESH_ID,
        )

    def chain(way, k, b):
        i = at[-k if way == 0 or k == 4 else k]
        if k < 3 or (k == 3 and (b < 2) == (way == 0)):
            back_z(i, b, way, k).wait_recv()
            dst = (RD, RU)[way]
            PART[i, b] = (
                PART[i, b].astype(jnp.float32) + dst[k, b].astype(jnp.float32)
            ).astype(jnp.bfloat16)
        start(back_z(i, b, way, k - 1))

    combine(7)
    for n in range(2):
        chain(0, 4, n)
        chain(1, 4, n + 2)
    for k in (3, 2, 1):
        for i in groups[k]:
            combine(i)
        for n in range(4):
            chain(0, k, (n + 2) % 4)
            chain(1, k, n)
    combine(0)
    for n in range(4):
        back_z(0, n, 0, 0).wait_recv()
        back_z(0, n, 1, 0).wait_recv()
        lanes = slice(n * WIDE, (n + 1) * WIDE)
        routed = (
            PART[0, n].astype(jnp.float32)
            + RD[0, n].astype(jnp.float32)
            + RU[0, n].astype(jnp.float32)
        )
        out_ref[:, lanes] = out_ref[:, lanes] + routed.astype(jnp.bfloat16).astype(jnp.float32)

    for copy in sends:
        copy.wait_send()
    for i in range(8):
        pieces_sent(i, OUT, asend)
        pieces_sent(i, EO, rsend)


def experts_layer(normed, hidden, tables, wg, wu, wd, sg, su, sd):
    vmem = pl.BlockSpec(memory_space=pltpu.VMEM)
    hbm = pl.BlockSpec(memory_space=pl.ANY)
    d, f = wg.shape
    bf = jnp.bfloat16
    return pl.pallas_call(
        moe_kernel,
        out_shape=jax.ShapeDtypeStruct((64, d), jnp.float32),
        in_specs=[vmem] * 3 + [hbm] * 6,
        out_specs=vmem,
        scratch_shapes=[
            pltpu.VMEM((8, SUBS, 64, WIDE), bf),
            pltpu.VMEM((8, 8, CAP, d), bf),
            pltpu.VMEM((8, 8, CAP, d), bf),
            pltpu.VMEM((8, 8, CAP, d), bf),
            pltpu.VMEM((8, 8, CAP, d), bf),
            pltpu.VMEM((8, SUBS, 64, WIDE), bf),
            pltpu.VMEM((4, SUBS, 64, WIDE), bf),
            pltpu.VMEM((4, SUBS, 64, WIDE), bf),
            pltpu.VMEM((d, f), bf),
            pltpu.VMEM((d, f), bf),
            pltpu.VMEM((f, d), bf),
            pltpu.VMEM((d, f), bf),
            pltpu.VMEM((d, f), bf),
            pltpu.VMEM((f, d), bf),
            pltpu.SemaphoreType.DMA((8, SUBS)),
            pltpu.SemaphoreType.DMA((8, SUBS)),
            pltpu.SemaphoreType.DMA((8,)),
            pltpu.SemaphoreType.DMA((8,)),
            pltpu.SemaphoreType.DMA((8,)),
            pltpu.SemaphoreType.DMA((8,)),
            pltpu.SemaphoreType.DMA((2, 4, SUBS)),
            pltpu.SemaphoreType.DMA((2, 4, SUBS)),
            pltpu.SemaphoreType.DMA((3,)),
            pltpu.SemaphoreType.DMA((6,)),
        ],
        compiler_params=pltpu.CompilerParams(
            collective_id=1, has_side_effects=True, vmem_limit_bytes=63 * 1024 * 1024
        ),
    )(normed, hidden, tables, wg, wu, wd, sg, su, sd)


def body(
    query_nope,
    query_rope,
    latent,
    key_rope,
    latent_gain,
    key_up,
    value_up,
    out_proj,
    residual,
    ffn_gain,
    expert_ids,
    route_weights,
    expert_gate,
    expert_up,
    expert_down,
    shared_gate,
    shared_up,
    shared_down,
):
    z, x, core, y = (lax.axis_index(n) for n in ("z", "x", "core", "y"))
    q_sp = (z * NX + x) * NC + core
    first_row = q_sp * ROWS
    positions = first_row + jnp.arange(ROWS, dtype=jnp.int32)

    normed_latent = scale_rows(latent, latent_gain)
    rot_key = rotate(key_rope[:, None, :], positions)[:, 0, :]
    packed = rot_key.reshape(2, 4, 32, ROPE).transpose(0, 2, 1, 3).reshape(2, 32, 256)
    payload = jnp.concatenate([normed_latent.reshape(2, 128, 256), packed], axis=1)

    key_local = lax.dynamic_slice_in_dim(key_up, y * 256, 256, 1)
    value_local = lax.dynamic_slice_in_dim(value_up, y * 256, 256, 1)
    rot_query = rotate(query_rope.reshape(ROWS, 2, ROPE), positions)
    q_cat = jnp.concatenate(
        [
            query_nope.reshape(ROWS, 2, NOPE),
            rot_query,
            jnp.zeros((ROWS, 2, 64), jnp.bfloat16),
        ],
        axis=-1,
    ).transpose(1, 0, 2)

    flat_ids = expert_ids.reshape(-1)
    onehot = (flat_ids[:, None] == jnp.arange(64, dtype=jnp.int32)[None, :]).astype(jnp.float32)
    earlier = (
        jnp.arange(256, dtype=jnp.int32)[None, :] < jnp.arange(256, dtype=jnp.int32)[:, None]
    ).astype(jnp.float32)
    before = jnp.dot(earlier, onehot)
    rank = jnp.sum(before * onehot, axis=1).reshape(64, 4)
    tables = jnp.concatenate([expert_ids.astype(jnp.float32) * CAP + rank, route_weights], axis=1)
    tables = jnp.concatenate([tables.T, jnp.zeros((8, 64), jnp.float32)], axis=1)
    hidden_one, normed, gathered = gather_attend(
        payload, tables, q_cat, key_local, value_local, out_proj, residual, ffn_gain
    )
    summed = experts_layer(
        normed, hidden_one, gathered, expert_gate[0], expert_up[0], expert_down[0],
        shared_gate, shared_up, shared_down,
    )
    return summed.astype(jnp.bfloat16)


def solution(mesh):
    fine = Mesh(mesh.devices.reshape(NZ, NX, NC, NY), ("z", "x", "core", "y"))
    sp = ("z", "x", "core")
    every = ("z", "x", "core", "y")
    in_specs = (
        P(sp, "y"),
        P(sp, "y"),
        P(sp, None),
        P(sp, None),
        P(),
        P(),
        P(),
        P("y", None),
        P(every, None),
        P(),
        P(every, None),
        P(every, None),
        P(sp, None, None),
        P(sp, None, None),
        P(sp, None, None),
        P(),
        P(),
        P(),
    )
    return jax.shard_map(
        body, mesh=fine, in_specs=in_specs, out_specs=P(every, None), check_vma=False
    )
```

```python
import math

import jax
import jax.numpy as jnp
from jax import lax
from jax.experimental import pallas as pl
from jax.experimental.pallas import tpu as pltpu
from jax.sharding import Mesh, PartitionSpec as P

NOPE = 128
ROPE = 64
VDIM = 128
NZ, NX, NC, NY = 8, 4, 2, 4
CAP = 8
ROWS = 256

rope_base = 10000.0
norm_eps = 1e-06


LOG2E = 1.4426950408889634
MESH_ID = pl.DeviceIdType.MESH
SUBS = 4
WIDE = 512
OFFS = (0, -1, 1, -2, 2, -3, 3, -4)
HALF = 160


def ring(value, size):
    return lax.rem(value + size, size)


def gather_attend_kernel(
    lat_ref, kr_ref, qn_ref, qr_ref, cos_ref, sin_ref, lg_ref, tab_ref, res_ref, fg_ref,
    ku_h, vu_h, op_ref, wg_h, wu_h, wd_h, sg_h, su_h, sd_h, out_ref,
    G, T, m_ref, l_ref, acc_ref, W, HS, HX, q_ref, ku_ref, vu_ref,
    HID, ACC, COL, OUT, ARR, EO, RET, PART, RD, RU, wg, wu, wd, sg, su, sd,
    recv, trecv, zsend, tsend, xsend, fsend, ysend, csend, lsem,
    wrecv, wsend, wfsend, wcsend, hrecv, hsend, usem, wsem,
    ezrecv, ezsend, arecv, asend, rrecv, rsend, drecv, dsend, elsem,
):
    z, x, c, y = (lax.axis_index(n) for n in ("z", "x", "core", "y"))
    hm = lax.rem(y, 2)
    ho = 1 - hm
    up, down = {"z": ring(z + 1, NZ)}, {"z": ring(z - 1, NZ)}
    right, left = {"x": ring(x + 1, NX)}, {"x": ring(x - 1, NX)}
    above, below = {"y": ring(y + 1, NY)}, {"y": ring(y - 1, NY)}
    mate = {"core": 1 - c}
    xs = {0: x, -1: ring(x - 1, NX), 1: ring(x + 1, NX), 2: ring(x + 2, NX)}
    ZZ = [ring(z + off, NZ) for off in OFFS]
    me = x * NC + c
    peers = []
    for q in range(1, 8):
        p = ring(me + q, 8)
        peers.append((p, {"x": p // NC, "core": lax.rem(p, NC)}))
    partners = [up, down, above, below] + [dev for _, dev in peers]
    barrier = pltpu.get_barrier_semaphore()
    for dev in partners:
        pl.semaphore_signal(barrier, inc=1, device_id=dev, device_id_type=MESH_ID)

    mine_cols = pl.ds(pl.multiple_of(y * 256, 256), 256)
    ups = [
        pltpu.make_async_copy(src.at[:, mine_cols], dst, usem.at[n])
        for n, (src, dst) in enumerate(((ku_h, ku_ref), (vu_h, vu_ref)))
    ]
    for copy in ups:
        copy.start()

    def piece(zz, xx, h, sem, dev):
        slot = G.at[c, zz, xx, h]
        return pltpu.make_async_remote_copy(
            src_ref=slot, dst_ref=slot, send_sem=sem, recv_sem=recv.at[c, zz, xx, h],
            device_id=dev, device_id_type=MESH_ID,
        )

    def arrived(par, zz, xx, h):
        slot = G.at[par, zz, xx, h]
        pltpu.make_async_remote_copy(
            src_ref=slot, dst_ref=slot, send_sem=csend, recv_sem=recv.at[par, zz, xx, h],
            device_id=mate, device_id_type=MESH_ID,
        ).wait_recv()

    sent = []

    def send(zz, xx, h, sems, at, dev):
        piece(zz, xx, h, sems.at[at], dev).start()
        sent.append(lambda: piece(zz, xx, h, sems.at[at], dev).wait_send())

    def to_mate(zz, xx, h):
        piece(zz, xx, h, csend, mate).start()

    def table(zz, sem, dev):
        return pltpu.make_async_remote_copy(
            src_ref=T.at[zz], dst_ref=T.at[zz], send_sem=sem, recv_sem=trecv.at[zz],
            device_id=dev, device_id_type=MESH_ID,
        )

    def send_table(zz, at, dev):
        table(zz, tsend.at[at], dev).start()
        sent.append(lambda: table(zz, tsend.at[at], dev).wait_send())

    def ev_z(i):
        off = OFFS[i]
        zz = ZZ[i]
        for h in range(2):
            if i > 0:
                arrived(c, zz, x, h)
            if -4 < off <= 0:
                send(zz, x, h, zsend, (0, -off, h), up)
            if 0 <= off < 3:
                send(zz, x, h, zsend, (1, off, h), down)
            to_mate(zz, x, h)
        send(zz, x, hm, xsend, (i, 0), right)
        send(zz, x, hm, xsend, (i, 1), left)
        if i > 0:
            table(zz, tsend.at[0, 0], up).wait_recv()
        if -4 < off <= 0:
            send_table(zz, (0, -off), up)
        if 0 <= off < 3:
            send_table(zz, (1, off), down)

    def to_y(i, j, zz, xx):
        send(zz, xx, hm, ysend, (i, j), above if (i + j) % 2 == 0 else below)

    def ev_x1(i):
        zz = ZZ[i]
        arrived(c, zz, xs[-1], hm)
        if i % 2 == 0:
            send(zz, xs[-1], hm, fsend, (i,), right)
        to_y(i, 0, zz, xs[-1])
        to_mate(zz, xs[-1], hm)
        arrived(c, zz, xs[1], hm)
        if i % 2 == 1:
            send(zz, xs[1], hm, fsend, (i,), left)
        to_y(i, 1, zz, xs[1])
        to_mate(zz, xs[1], hm)

    def ev_x2(i):
        zz = ZZ[i]
        arrived(c, zz, xs[2], hm)
        to_y(i, 2, zz, xs[2])
        to_mate(zz, xs[2], hm)

    def ev_y(i, dx):
        zz = ZZ[i]
        arrived(c, zz, xs[dx], ho)
        to_mate(zz, xs[dx], ho)

    yb, ya, y2 = ring(y - 1, NY), ring(y + 1, NY), ring(y + 2, NY)

    def proj(yy, r, sem, dev):
        slot = W.at[yy, c, r]
        return pltpu.make_async_remote_copy(
            src_ref=slot, dst_ref=slot, send_sem=sem, recv_sem=wrecv.at[yy, c, r],
            device_id=dev, device_id_type=MESH_ID,
        )

    def proj_in(yy, half, r):
        slot = W.at[yy, half, r]
        pltpu.make_async_remote_copy(
            src_ref=slot, dst_ref=slot, send_sem=wcsend, recv_sem=wrecv.at[yy, half, r],
            device_id=mate, device_id_type=MESH_ID,
        ).wait_recv()

    def proj_send(yy, r, sems, where, dev):
        proj(yy, r, sems.at[where], dev).start()
        sent.append(lambda: proj(yy, r, sems.at[where], dev).wait_send())

    def ev_proj(r):
        proj_send(y, r, wsend, (0, r), above)
        proj_send(y, r, wsend, (1, r), below)

    def ev_proj1(r):
        proj_in(yb, c, r)
        if r % 2 == 0:
            proj_send(yb, r, wfsend, (r,), above)
        proj(yb, r, wcsend, mate).start()
        proj_in(ya, c, r)
        if r % 2 == 1:
            proj_send(ya, r, wfsend, (r,), below)
        proj(ya, r, wcsend, mate).start()

    def ev_proj2(r):
        proj_in(y2, c, r)
        proj(y2, r, wcsend, mate).start()

    own_proj = [
        pltpu.make_async_copy(
            op_ref.at[:, :, half * 1024 : (half + 1) * 1024], W.at[y, half], lsem.at[2 + half]
        )
        for half in range(2)
    ]
    for copy in own_proj:
        copy.start()
    lane = lax.broadcasted_iota(jnp.int32, (1, 128), 1)

    def turn(values):
        ahead, behind = pltpu.roll(values, 96, 1), pltpu.roll(values, 32, 1)
        other = jnp.where(lane % 64 < 32, ahead, behind)
        return values * cos_ref[...] + other * sin_ref[...]

    lat = lat_ref[...].astype(jnp.float32)
    factor = lax.rsqrt(jnp.sum(lat * lat, axis=1, keepdims=True) * (1.0 / 256) + norm_eps)
    lat = (lat * factor * lg_ref[...].astype(jnp.float32)).astype(jnp.bfloat16)
    keys_rope = kr_ref[...].astype(jnp.float32)
    keys_rope = turn(jnp.concatenate([keys_rope, keys_rope], axis=1))
    for h in range(2):
        G[c, z, x, h, 0:128, :] = lat[h * 128 : (h + 1) * 128]
        for n in range(2):
            lo = h * 128 + n * 64
            both = jnp.where(lane < 64, keys_rope[lo : lo + 32], keys_rope[lo + 32 : lo + 64])
            G[c, z, x, h, 128:HALF, n * 128 : (n + 1) * 128] = both.astype(jnp.bfloat16)
    T[z] = tab_ref[...]
    pl.semaphore_wait(barrier, len(partners))

    weights = [
        pltpu.make_async_copy(src, dst, wsem.at[n])
        for n, (src, dst) in enumerate(
            ((wg_h, wg), (wu_h, wu), (wd_h, wd), (sg_h, sg), (su_h, su), (sd_h, sd))
        )
    ]

    turned = turn(qr_ref[...].astype(jnp.float32)).astype(jnp.bfloat16)

    def prepare():
        for h in range(2):
            q_ref[h] = jnp.concatenate(
                [
                    qn_ref[:, h * NOPE : (h + 1) * NOPE],
                    turned[:, h * ROPE : (h + 1) * ROPE],
                    jnp.zeros((ROWS, 64), jnp.bfloat16),
                ],
                axis=1,
            )
        for copy in ups:
            copy.wait()
        for w in weights:
            w.start()
        m_ref[...] = jnp.full(m_ref.shape, -1e30, jnp.float32)
        l_ref[...] = jnp.zeros(l_ref.shape, jnp.float32)
        acc_ref[...] = jnp.zeros(acc_ref.shape, jnp.float32)

    scale = LOG2E / math.sqrt(NOPE + ROPE)
    keys = 512

    def compute(zz, xx, masked):
        lat = jnp.concatenate(
            [G[par, zz, xx, h, 0:128, :] for par in range(2) for h in range(2)], axis=0
        )
        rope = jnp.concatenate(
            [
                G[par, zz, xx, h, 128:HALF, g * ROPE : (g + 1) * ROPE]
                for par in range(2)
                for h in range(2)
                for g in range(4)
            ],
            axis=0,
        )
        rope = jnp.concatenate([rope, jnp.zeros((keys, ROPE), jnp.bfloat16)], axis=1)
        k = jnp.dot(lat, ku_ref[...], preferred_element_type=jnp.float32).astype(jnp.bfloat16)
        v = jnp.dot(lat, vu_ref[...], preferred_element_type=jnp.float32).astype(jnp.bfloat16)
        if masked:
            kpos = lax.broadcasted_iota(jnp.int32, (1, keys), 1)
            qpos = c * ROWS + lax.broadcasted_iota(jnp.int32, (ROWS, 1), 0)
            allowed = kpos <= qpos
        for h in range(2):
            kcat = jnp.concatenate([k[:, h * NOPE : (h + 1) * NOPE], rope], axis=1)
            s = lax.dot_general(
                q_ref[h], kcat, (((1,), (1,)), ((), ())), preferred_element_type=jnp.float32
            )
            s = s * scale
            if masked:
                s = jnp.where(allowed, s, -1e30)
            m_old = m_ref[h]
            m_new = jnp.maximum(m_old, jnp.max(s, axis=1, keepdims=True))
            p = jnp.exp2(s - m_new[:, :1])
            if masked:
                p = jnp.where(allowed, p, 0.0)
            alpha = jnp.exp2(m_old - m_new)
            l_ref[h] = l_ref[h] * alpha + jnp.sum(p, axis=1, keepdims=True)
            acc_ref[h] = acc_ref[h] * alpha + jnp.dot(
                p.astype(jnp.bfloat16),
                v[:, h * VDIM : (h + 1) * VDIM],
                preferred_element_type=jnp.float32,
            )
            m_ref[h] = m_new

    mine = z * NX + x

    def round_(s, carry):
        for k in range(13):

            @pl.when(s == k)
            def _():
                if k < 8:
                    ev_z(k)
                if k == 0:
                    prepare()
                if 0 <= k - 1 < 8:
                    ev_x1(k - 1)
                if 0 <= k - 2 < 8:
                    ev_x2(k - 2)
                if 0 <= k - 3 < 8:
                    ev_y(k - 3, -1)
                    ev_y(k - 3, 1)
                if 0 <= k - 4 < 8:
                    ev_y(k - 4, 2)
                if k == 1:
                    for copy in own_proj:
                        copy.wait()
                if 0 <= k - 1 < 8:
                    ev_proj(k - 1)
                if 0 <= k - 3 < 8:
                    ev_proj1(k - 3)
                if 0 <= k - 5 < 8:
                    ev_proj2(k - 5)

        def pair(d, carry):
            i = s - 1 - jnp.where(d == 0, 0, jnp.where(d == 3, 4, 3))

            @pl.when((i >= 0) & (i < 8))
            def _():
                off = jnp.where(lax.rem(i, 2) == 1, -((i + 1) // 2), i // 2)
                dx = jnp.where(d == 3, 2, jnp.where(d == 1, -1, jnp.where(d == 2, 1, 0)))
                zz = ring(z + off, NZ)
                xx = ring(x + dx, NX)
                for h in range(2):
                    arrived(1 - c, zz, xx, h)
                theirs = zz * NX + xx

                @pl.when(theirs < mine)
                def _():
                    compute(zz, xx, False)

                @pl.when(theirs == mine)
                def _():
                    compute(zz, xx, True)

            return carry

        return lax.fori_loop(0, 4, pair, carry)

    lax.fori_loop(0, 13, round_, 0)

    for h in range(2):
        heads = (acc_ref[h] / l_ref[h]).astype(jnp.bfloat16)
        for q in range(NY):
            HS[q, :, h * VDIM : (h + 1) * VDIM] = heads[q * 64 : (q + 1) * 64]

    def heads_to(yy):
        return pltpu.make_async_remote_copy(
            src_ref=HS.at[yy], dst_ref=HX.at[y], send_sem=hsend.at[yy], recv_sem=hrecv.at[y],
            device_id={"y": yy}, device_id_type=MESH_ID,
        )

    for yy in (y2, ya, yb):
        heads_to(yy).start()
    HX[y] = HS[y]
    for yy in (yb, ya, y2):
        for r in range(8):
            proj_in(yy, 1 - c, r)
    for yy in (yb, ya, y2):
        pltpu.make_async_remote_copy(
            src_ref=HS.at[yy], dst_ref=HX.at[yy], send_sem=hsend.at[yy], recv_sem=hrecv.at[yy],
            device_id={"y": yy}, device_id_type=MESH_ID,
        ).wait_recv()
    squares = jnp.zeros((64, 1), jnp.float32)
    for half in range(2):
        lanes = slice(half * 1024, (half + 1) * 1024)
        total = jnp.zeros((64, 1024), jnp.float32)
        for q in range(NY):
            weight = jnp.concatenate([W[q, half, r] for r in range(8)], axis=0)
            rows = jnp.dot(HX[q], weight, preferred_element_type=jnp.float32)
            total = total + rows.astype(jnp.bfloat16).astype(jnp.float32)
        one = (res_ref[:, lanes].astype(jnp.float32) + total).astype(jnp.bfloat16)
        HID[:, lanes] = one
        one = one.astype(jnp.float32)
        squares = squares + jnp.sum(one * one, axis=1, keepdims=True)
    factor = lax.rsqrt(squares * (1.0 / 2048) + norm_eps)
    for b in range(SUBS):
        lanes = slice(b * WIDE, (b + 1) * WIDE)
        COL[0, b] = (
            HID[:, lanes].astype(jnp.float32) * factor * fg_ref[:, lanes].astype(jnp.float32)
        ).astype(jnp.bfloat16)
    experts_part(
        z, x, c, y, up, down, peers, weights, out_ref,
        T, HID, ACC, COL, OUT, ARR, EO, RET, PART, RD, RU, wg, wu, wd, sg, su, sd,
        ezrecv, ezsend, arecv, asend, rrecv, rsend, drecv, dsend, elsem,
    )
    for yy in (y2, ya, yb):
        heads_to(yy).wait_send()
    pltpu.make_async_remote_copy(
        src_ref=W.at[0:3, 0], dst_ref=W.at[0:3, 0], send_sem=wcsend, recv_sem=wrecv.at[0, 0, 0],
        device_id=mate, device_id_type=MESH_ID,
    ).wait_send()
    for wait in sent:
        wait()
    whole = G.at[c]
    pltpu.make_async_remote_copy(
        src_ref=whole, dst_ref=whole, send_sem=csend, recv_sem=recv.at[0, 0, 0, 0],
        device_id=mate, device_id_type=MESH_ID,
    ).wait_send()


def layer(small, large):
    vmem = pl.BlockSpec(memory_space=pltpu.VMEM)
    hbm = pl.BlockSpec(memory_space=pl.ANY)
    bf, f32, dma = jnp.bfloat16, jnp.float32, pltpu.SemaphoreType.DMA
    d, f = large[3].shape
    shapes = [
        ((2, NZ, NX, 2, HALF, 256), bf),
        ((NZ, 8, 128), f32),
        ((2, ROWS, 128), f32),
        ((2, ROWS, 128), f32),
        ((2, ROWS, 128), f32),
        ((NY, 2, 8, 32, 1024), bf),
        ((NY, 64, 256), bf),
        ((NY, 64, 256), bf),
        ((2, ROWS, 256), bf),
        ((256, 256), bf),
        ((256, 256), bf),
        ((64, d), bf),
        ((64, d), f32),
        ((8, SUBS, 64, WIDE), bf),
        ((8, 8, CAP, d), bf),
        ((8, 8, CAP, d), bf),
        ((8, 8, CAP, d), bf),
        ((8, 8, CAP, d), bf),
        ((8, SUBS, 64, WIDE), bf),
        ((4, SUBS, 64, WIDE), bf),
        ((4, SUBS, 64, WIDE), bf),
        ((d, f), bf),
        ((d, f), bf),
        ((f, d), bf),
        ((d, f), bf),
        ((d, f), bf),
        ((f, d), bf),
    ]
    sems = [
        (2, NZ, NX, 2), (NZ,), (2, 4, 2), (2, 4), (8, 2), (8,), (8, 3), (), (4,),
        (NY, 2, 8), (2, 8), (8,), (), (NY,), (NY,), (2,), (6,),
        (8, SUBS), (8, SUBS), (8,), (8,), (8,), (8,), (2, 4, SUBS), (2, 4, SUBS), (3,),
    ]
    return pl.pallas_call(
        gather_attend_kernel,
        out_shape=jax.ShapeDtypeStruct((64, 2048), jnp.bfloat16),
        in_specs=[vmem] * len(small) + [hbm] * len(large),
        out_specs=vmem,
        scratch_shapes=[pltpu.VMEM(*shape) for shape in shapes]
        + [dma(shape) if shape else dma for shape in sems],
        compiler_params=pltpu.CompilerParams(
            collective_id=0, has_side_effects=True, vmem_limit_bytes=63 * 1024 * 1024
        ),
    )(*small, *large)


def experts_part(
    z, x, c, y, up, down, peers, weights, out_ref,
    T, HID, ACC, COL, OUT, ARR, EO, RET, PART, RD, RU, wg, wu, wd, sg, su, sd,
    zrecv, zsend, arecv, asend, rrecv, rsend, drecv, dsend, lsem,
):
    me = x * NC + c

    at = {off: i for i, off in enumerate(OFFS)}

    def along_z(i, b, dev, off_to, n):
        there = at[off_to]
        return pltpu.make_async_remote_copy(
            src_ref=COL.at[i, b], dst_ref=COL.at[there, b], send_sem=zsend.at[n, b],
            recv_sem=zrecv.at[there, b], device_id=dev, device_id_type=MESH_ID,
        )

    def pass_on(off, b):
        i = at[off]
        if off != 0:
            along_z(i, b, up, off, 0).wait_recv()
        if -3 < off <= 0 or (off == -3 and b < 2):
            start(along_z(i, b, up, off - 1, -off))
        if 0 <= off < 3:
            start(along_z(i, b, down, off + 1, 4 + off))
        if off == 3 and b >= 2:
            start(along_z(i, b, down, -4, 7))

    sends = []

    def start(copy):
        copy.start()
        sends.append(copy)

    def pieces(i, src, dst, sems_send, sems_recv):
        for p, dev in peers:
            pltpu.make_async_remote_copy(
                src_ref=src.at[i, p], dst_ref=dst.at[i, me], send_sem=sems_send.at[i],
                recv_sem=sems_recv.at[i], device_id=dev, device_id_type=MESH_ID,
            ).start()
        pltpu.make_async_copy(src.at[i, me], dst.at[i, me], lsem.at[1]).start()
        pltpu.make_async_copy(src.at[i, me], dst.at[i, me], lsem.at[1]).wait()

    def pieces_in(i, dst, sems_recv):
        ref = dst.at[i, 0:7]
        pltpu.make_async_remote_copy(
            src_ref=ref, dst_ref=ref, send_sem=lsem.at[2], recv_sem=sems_recv.at[i],
            device_id=peers[0][1], device_id_type=MESH_ID,
        ).wait_recv()

    def pieces_sent(i, src, sems_send):
        ref = src.at[i, 0:7]
        pltpu.make_async_remote_copy(
            src_ref=ref, dst_ref=ref, send_sem=sems_send.at[i], recv_sem=lsem.at[2],
            device_id=peers[0][1], device_id_type=MESH_ID,
        ).wait_send()

    slots = lax.broadcasted_iota(jnp.int32, (64, 64), 0).astype(jnp.float32)

    def matches(i):
        tab = T[ring(z + OFFS[i], NZ)]
        base = (z * 64).astype(jnp.float32)
        return [(tab[k : k + 1, 0:64] - base) == slots for k in range(4)], tab

    def picks(i):
        hit, _ = matches(i)
        return jnp.where(hit[0] | hit[1] | hit[2] | hit[3], 1.0, 0.0).astype(jnp.bfloat16)

    def select(i, b, pick):
        rows = jnp.dot(pick, COL[i, b], preferred_element_type=jnp.float32)
        for p in range(8):
            OUT[i, p, :, b * WIDE : (b + 1) * WIDE] = rows[p * CAP : (p + 1) * CAP].astype(
                jnp.bfloat16
            )

    def gated(rows, gate, upper, lower):
        g = jnp.dot(rows, gate[...], preferred_element_type=jnp.float32)
        u = jnp.dot(rows, upper[...], preferred_element_type=jnp.float32)
        hidden = (g / (1.0 + jnp.exp(-g)) * u).astype(jnp.bfloat16)
        return jnp.dot(hidden, lower[...], preferred_element_type=jnp.float32)

    def expert(group):
        for i in group:
            pieces_in(i, ARR, arecv)
        rows = jnp.concatenate(
            [ARR[i, p].astype(jnp.float32) for i in group for p in range(8)], axis=0
        ).astype(jnp.bfloat16)
        done = gated(rows, wg, wu, wd)
        for n, i in enumerate(group):
            for p in range(8):
                lo = (n * 8 + p) * CAP
                EO[i, p] = done[lo : lo + CAP].astype(jnp.bfloat16)

    def combine(i):
        pieces_in(i, RET, rrecv)
        hit, tab = matches(i)
        share = jnp.zeros((64, 64), jnp.float32)
        for k in range(4):
            share = share + jnp.where(hit[k], tab[4 + k : 5 + k, 0:64], 0.0)
        hi = share.astype(jnp.bfloat16)
        lo = (share - hi.astype(jnp.float32)).astype(jnp.bfloat16)
        back = jnp.concatenate(
            [RET[i, p].astype(jnp.float32) for p in range(8)], axis=0
        ).astype(jnp.bfloat16)
        dims = (((0,), (0,)), ((), ()))
        total = lax.dot_general(hi, back, dims, preferred_element_type=jnp.float32)
        total = total + lax.dot_general(lo, back, dims, preferred_element_type=jnp.float32)
        for b in range(SUBS):
            PART[i, b] = total[:, b * WIDE : (b + 1) * WIDE].astype(jnp.bfloat16)

    groups = ((0,), (1, 2), (3, 4), (5, 6), (7,))

    def shared():
        for w in weights[3:]:
            w.wait()
        rows = jnp.concatenate([COL[0, b] for b in range(SUBS)], axis=1)
        ACC[...] = (
            HID[...].astype(jnp.float32)
            + gated(rows, sg, su, sd).astype(jnp.bfloat16).astype(jnp.float32)
        )

    def between(s, b):
        if s >= 2 and b == 1:
            if s == 2:
                for w in weights[:3]:
                    w.wait()
            expert(groups[s - 2])

    for s in range(5):
        pick = [picks(i) for i in groups[s]]
        for b in range(SUBS):
            for n, i in enumerate(groups[s]):
                pass_on(OFFS[i], b)
            for n, i in enumerate(groups[s]):
                select(i, b, pick[n])
            between(s, b)
        for i in groups[s]:
            pieces(i, OUT, ARR, asend, arecv)
    expert(groups[3])
    expert(groups[4])
    for group in reversed(groups):
        for i in group:
            pieces(i, EO, RET, rsend, rrecv)
    shared()

    def back_z(i, b, way, k):
        dst, dev = ((RD, down), (RU, up))[way]
        return pltpu.make_async_remote_copy(
            src_ref=PART.at[i, b], dst_ref=dst.at[k, b], send_sem=dsend.at[way, k, b],
            recv_sem=drecv.at[way, k, b], device_id=dev, device_id_type=MESH_ID,
        )

    def chain(way, k, b):
        i = at[-k if way == 0 or k == 4 else k]
        if k < 3 or (k == 3 and (b < 2) == (way == 0)):
            back_z(i, b, way, k).wait_recv()
            dst = (RD, RU)[way]
            PART[i, b] = (
                PART[i, b].astype(jnp.float32) + dst[k, b].astype(jnp.float32)
            ).astype(jnp.bfloat16)
        start(back_z(i, b, way, k - 1))

    combine(7)
    for n in range(2):
        chain(0, 4, n)
        chain(1, 4, n + 2)
    for k in (3, 2, 1):
        for i in groups[k]:
            combine(i)
        for n in range(4):
            chain(0, k, (n + 2) % 4)
            chain(1, k, n)
    combine(0)
    for n in range(4):
        back_z(0, n, 0, 0).wait_recv()
        back_z(0, n, 1, 0).wait_recv()
        lanes = slice(n * WIDE, (n + 1) * WIDE)
        routed = (
            PART[0, n].astype(jnp.float32)
            + RD[0, n].astype(jnp.float32)
            + RU[0, n].astype(jnp.float32)
        )
        total = ACC[:, lanes] + routed.astype(jnp.bfloat16).astype(jnp.float32)
        out_ref[:, lanes] = total.astype(jnp.bfloat16)

    for copy in sends:
        copy.wait_send()
    for i in range(8):
        pieces_sent(i, OUT, asend)
        pieces_sent(i, EO, rsend)


def body(
    query_nope,
    query_rope,
    latent,
    key_rope,
    latent_gain,
    key_up,
    value_up,
    out_proj,
    residual,
    ffn_gain,
    expert_ids,
    route_weights,
    expert_gate,
    expert_up,
    expert_down,
    shared_gate,
    shared_up,
    shared_down,
):
    z, x, core, y = (lax.axis_index(n) for n in ("z", "x", "core", "y"))
    q_sp = (z * NX + x) * NC + core
    first_row = q_sp * ROWS
    positions = first_row + jnp.arange(ROWS, dtype=jnp.int32)
    half_dim = ROPE // 2
    frequency = rope_base ** (-jnp.arange(half_dim, dtype=jnp.float32) / half_dim)
    angles = positions.astype(jnp.float32)[:, None] * jnp.concatenate([frequency] * 4)[None, :]
    sign = jnp.where(jnp.arange(128) % ROPE < half_dim, -1.0, 1.0)
    cosine, sine_part = jnp.cos(angles), jnp.sin(angles) * sign[None, :]

    flat_ids = expert_ids.reshape(-1)
    onehot = (flat_ids[:, None] == jnp.arange(64, dtype=jnp.int32)[None, :]).astype(jnp.float32)
    earlier = (
        jnp.arange(256, dtype=jnp.int32)[None, :] < jnp.arange(256, dtype=jnp.int32)[:, None]
    ).astype(jnp.float32)
    before = jnp.dot(earlier, onehot)
    rank = jnp.sum(before * onehot, axis=1).reshape(64, 4)
    tables = jnp.concatenate([expert_ids.astype(jnp.float32) * CAP + rank, route_weights], axis=1)
    tables = jnp.concatenate([tables.T, jnp.zeros((8, 64), jnp.float32)], axis=1)
    small = (
        latent, key_rope, query_nope, query_rope, cosine, sine_part, latent_gain.reshape(1, 256),
        tables, residual, ffn_gain.reshape(1, 2048),
    )
    large = (
        key_up, value_up, out_proj.reshape(8, 32, 2048), expert_gate[0], expert_up[0],
        expert_down[0], shared_gate, shared_up, shared_down,
    )
    return layer(small, large)


def solution(mesh):
    fine = Mesh(mesh.devices.reshape(NZ, NX, NC, NY), ("z", "x", "core", "y"))
    sp = ("z", "x", "core")
    every = ("z", "x", "core", "y")
    in_specs = (
        P(sp, "y"),
        P(sp, "y"),
        P(sp, None),
        P(sp, None),
        P(),
        P(),
        P(),
        P("y", None),
        P(every, None),
        P(),
        P(every, None),
        P(every, None),
        P(sp, None, None),
        P(sp, None, None),
        P(sp, None, None),
        P(),
        P(),
        P(),
    )
    return jax.shard_map(
        body, mesh=fine, in_specs=in_specs, out_specs=P(every, None), check_vma=False
    )
```

```python
import math

import jax
import jax.numpy as jnp
from jax import lax
from jax.experimental import pallas as pl
from jax.experimental.pallas import tpu as pltpu
from jax.sharding import Mesh, PartitionSpec as P

NOPE = 128
ROPE = 64
VDIM = 128
NZ, NX, NC, NY = 8, 4, 2, 4
CAP = 8
ROWS = 256

rope_base = 10000.0
norm_eps = 1e-06


LOG2E = 1.4426950408889634
MESH_ID = pl.DeviceIdType.MESH
SUBS = 4
WIDE = 512
OFFS = (0, -1, 1, -2, 2, -3, 3, -4)
HALF = 160


def ring(value, size):
    return lax.rem(value + size, size)


def gather_attend_kernel(
    lat_ref, kr_ref, qn_ref, qr_ref, cos_ref, sin_ref, lg_ref, ids_ref, rw_ref, res_ref, fg_ref,
    ku_h, vu_h, op_ref, wg_h, wu_h, wd_h, sg_h, su_h, sd_h, out_ref,
    G, T, m_ref, l_ref, acc_ref, W, HS, HX, q_ref, ku_ref, vu_ref,
    HID, ACC, COL, OUT, ARR, EO, RET, PART, RD, RU, wg, wu, wd, sg, su, sd,
    recv, trecv, zsend, tsend, xsend, fsend, ysend, csend, lsem,
    wrecv, wsend, wfsend, wcsend, hrecv, hsend, usem, wsem,
    ezrecv, ezsend, arecv, asend, rrecv, rsend, drecv, dsend, elsem,
):
    z, x, c, y = (lax.axis_index(n) for n in ("z", "x", "core", "y"))
    hm = lax.rem(y, 2)
    ho = 1 - hm
    up, down = {"z": ring(z + 1, NZ)}, {"z": ring(z - 1, NZ)}
    right, left = {"x": ring(x + 1, NX)}, {"x": ring(x - 1, NX)}
    above, below = {"y": ring(y + 1, NY)}, {"y": ring(y - 1, NY)}
    mate = {"core": 1 - c}
    xs = {0: x, -1: ring(x - 1, NX), 1: ring(x + 1, NX), 2: ring(x + 2, NX)}
    ZZ = [ring(z + off, NZ) for off in OFFS]
    me = x * NC + c
    peers = []
    for q in range(1, 8):
        p = ring(me + q, 8)
        peers.append((p, {"x": p // NC, "core": lax.rem(p, NC)}))
    partners = [up, down, above, below] + [dev for _, dev in peers]
    barrier = pltpu.get_barrier_semaphore()
    for dev in partners:
        pl.semaphore_signal(barrier, inc=1, device_id=dev, device_id_type=MESH_ID)

    mine_cols = pl.ds(pl.multiple_of(y * 256, 256), 256)
    ups = [
        pltpu.make_async_copy(src.at[:, mine_cols], dst, usem.at[n])
        for n, (src, dst) in enumerate(((ku_h, ku_ref), (vu_h, vu_ref)))
    ]
    for copy in ups:
        copy.start()

    def piece(zz, xx, h, sem, dev):
        slot = G.at[c, zz, xx, h]
        return pltpu.make_async_remote_copy(
            src_ref=slot, dst_ref=slot, send_sem=sem, recv_sem=recv.at[c, zz, xx, h],
            device_id=dev, device_id_type=MESH_ID,
        )

    def arrived(par, zz, xx, h):
        slot = G.at[par, zz, xx, h]
        pltpu.make_async_remote_copy(
            src_ref=slot, dst_ref=slot, send_sem=csend, recv_sem=recv.at[par, zz, xx, h],
            device_id=mate, device_id_type=MESH_ID,
        ).wait_recv()

    sent = []

    def send(zz, xx, h, sems, at, dev):
        piece(zz, xx, h, sems.at[at], dev).start()
        sent.append(lambda: piece(zz, xx, h, sems.at[at], dev).wait_send())

    def to_mate(zz, xx, h):
        piece(zz, xx, h, csend, mate).start()

    def table(zz, sem, dev):
        return pltpu.make_async_remote_copy(
            src_ref=T.at[zz], dst_ref=T.at[zz], send_sem=sem, recv_sem=trecv.at[zz],
            device_id=dev, device_id_type=MESH_ID,
        )

    def send_table(zz, at, dev):
        table(zz, tsend.at[at], dev).start()
        sent.append(lambda: table(zz, tsend.at[at], dev).wait_send())

    def ev_z(i):
        off = OFFS[i]
        zz = ZZ[i]
        for h in range(2):
            if i > 0:
                arrived(c, zz, x, h)
            if -4 < off <= 0:
                send(zz, x, h, zsend, (0, -off, h), up)
            if 0 <= off < 3:
                send(zz, x, h, zsend, (1, off, h), down)
            to_mate(zz, x, h)
        send(zz, x, hm, xsend, (i, 0), right)
        send(zz, x, hm, xsend, (i, 1), left)
        if i > 0:
            table(zz, tsend.at[0, 0], up).wait_recv()
        if -4 < off <= 0:
            send_table(zz, (0, -off), up)
        if 0 <= off < 3:
            send_table(zz, (1, off), down)

    def to_y(i, j, zz, xx):
        send(zz, xx, hm, ysend, (i, j), above if (i + j) % 2 == 0 else below)

    def ev_x1(i):
        zz = ZZ[i]
        arrived(c, zz, xs[-1], hm)
        if i % 2 == 0:
            send(zz, xs[-1], hm, fsend, (i,), right)
        to_y(i, 0, zz, xs[-1])
        to_mate(zz, xs[-1], hm)
        arrived(c, zz, xs[1], hm)
        if i % 2 == 1:
            send(zz, xs[1], hm, fsend, (i,), left)
        to_y(i, 1, zz, xs[1])
        to_mate(zz, xs[1], hm)

    def ev_x2(i):
        zz = ZZ[i]
        arrived(c, zz, xs[2], hm)
        to_y(i, 2, zz, xs[2])
        to_mate(zz, xs[2], hm)

    def ev_y(i, dx):
        zz = ZZ[i]
        arrived(c, zz, xs[dx], ho)
        to_mate(zz, xs[dx], ho)

    yb, ya, y2 = ring(y - 1, NY), ring(y + 1, NY), ring(y + 2, NY)

    def proj(yy, r, sem, dev):
        slot = W.at[yy, c, r]
        return pltpu.make_async_remote_copy(
            src_ref=slot, dst_ref=slot, send_sem=sem, recv_sem=wrecv.at[yy, c, r],
            device_id=dev, device_id_type=MESH_ID,
        )

    def proj_in(yy, half, r):
        slot = W.at[yy, half, r]
        pltpu.make_async_remote_copy(
            src_ref=slot, dst_ref=slot, send_sem=wcsend, recv_sem=wrecv.at[yy, half, r],
            device_id=mate, device_id_type=MESH_ID,
        ).wait_recv()

    def proj_send(yy, r, sems, where, dev):
        proj(yy, r, sems.at[where], dev).start()
        sent.append(lambda: proj(yy, r, sems.at[where], dev).wait_send())

    def ev_proj(r):
        proj_send(y, r, wsend, (0, r), above)
        proj_send(y, r, wsend, (1, r), below)

    def ev_proj1(r):
        proj_in(yb, c, r)
        if r % 2 == 0:
            proj_send(yb, r, wfsend, (r,), above)
        proj(yb, r, wcsend, mate).start()
        proj_in(ya, c, r)
        if r % 2 == 1:
            proj_send(ya, r, wfsend, (r,), below)
        proj(ya, r, wcsend, mate).start()

    def ev_proj2(r):
        proj_in(y2, c, r)
        proj(y2, r, wcsend, mate).start()

    own_proj = [
        pltpu.make_async_copy(
            op_ref.at[:, :, half * 1024 : (half + 1) * 1024], W.at[y, half], lsem.at[2 + half]
        )
        for half in range(2)
    ]
    for copy in own_proj:
        copy.start()
    lane = lax.broadcasted_iota(jnp.int32, (1, 128), 1)

    def turn(values):
        ahead, behind = pltpu.roll(values, 96, 1), pltpu.roll(values, 32, 1)
        other = jnp.where(lane % 64 < 32, ahead, behind)
        return values * cos_ref[...] + other * sin_ref[...]

    lat = lat_ref[...].astype(jnp.float32)
    factor = lax.rsqrt(jnp.sum(lat * lat, axis=1, keepdims=True) * (1.0 / 256) + norm_eps)
    lat = (lat * factor * lg_ref[...].astype(jnp.float32).reshape(1, 256)).astype(jnp.bfloat16)
    keys_rope = kr_ref[...].astype(jnp.float32).T
    keys_rope = turn(jnp.concatenate([keys_rope, keys_rope], axis=1))
    for h in range(2):
        G[c, z, x, h, 0:128, :] = lat[h * 128 : (h + 1) * 128]
        for n in range(2):
            lo = h * 128 + n * 64
            both = jnp.where(lane < 64, keys_rope[lo : lo + 32], keys_rope[lo + 32 : lo + 64])
            G[c, z, x, h, 128:HALF, n * 128 : (n + 1) * 128] = both.astype(jnp.bfloat16)
    ids = ids_ref[...].astype(jnp.float32)
    expert = lax.broadcasted_iota(jnp.int32, (64, 64), 0).astype(jnp.float32)
    named = [jnp.where(ids[k : k + 1] == expert, 1.0, 0.0) for k in range(4)]
    earlier = jnp.where(
        lax.broadcasted_iota(jnp.int32, (64, 64), 0) < lax.broadcasted_iota(jnp.int32, (64, 64), 1),
        1.0,
        0.0,
    )
    before = jnp.dot(
        (named[0] + named[1] + named[2] + named[3]).astype(jnp.bfloat16),
        earlier.astype(jnp.bfloat16),
        preferred_element_type=jnp.float32,
    )
    rank = [jnp.sum(one * before, axis=0, keepdims=True) for one in named]
    table_rows = jnp.concatenate([ids * CAP + jnp.concatenate(rank, axis=0), rw_ref[...]], axis=0)
    T[z] = jnp.concatenate([table_rows, jnp.zeros((8, 64), jnp.float32)], axis=1)
    pl.semaphore_wait(barrier, len(partners))

    weights = [
        pltpu.make_async_copy(src, dst, wsem.at[n])
        for n, (src, dst) in enumerate(
            ((wg_h, wg), (wu_h, wu), (wd_h, wd), (sg_h, sg), (su_h, su), (sd_h, sd))
        )
    ]

    turned = turn(qr_ref[...].astype(jnp.float32)).astype(jnp.bfloat16)

    def prepare():
        for h in range(2):
            q_ref[h] = jnp.concatenate(
                [
                    qn_ref[:, h * NOPE : (h + 1) * NOPE],
                    turned[:, h * ROPE : (h + 1) * ROPE],
                    jnp.zeros((ROWS, 64), jnp.bfloat16),
                ],
                axis=1,
            )
        for copy in ups:
            copy.wait()
        for w in weights:
            w.start()
        m_ref[...] = jnp.full(m_ref.shape, -1e30, jnp.float32)
        l_ref[...] = jnp.zeros(l_ref.shape, jnp.float32)
        acc_ref[...] = jnp.zeros(acc_ref.shape, jnp.float32)

    scale = LOG2E / math.sqrt(NOPE + ROPE)
    keys = 512

    def compute(zz, xx, masked):
        lat = jnp.concatenate(
            [G[par, zz, xx, h, 0:128, :] for par in range(2) for h in range(2)], axis=0
        )
        rope = jnp.concatenate(
            [
                G[par, zz, xx, h, 128:HALF, g * ROPE : (g + 1) * ROPE]
                for par in range(2)
                for h in range(2)
                for g in range(4)
            ],
            axis=0,
        )
        rope = jnp.concatenate([rope, jnp.zeros((keys, ROPE), jnp.bfloat16)], axis=1)
        k = jnp.dot(lat, ku_ref[...], preferred_element_type=jnp.float32).astype(jnp.bfloat16)
        v = jnp.dot(lat, vu_ref[...], preferred_element_type=jnp.float32).astype(jnp.bfloat16)
        if masked:
            kpos = lax.broadcasted_iota(jnp.int32, (1, keys), 1)
            qpos = c * ROWS + lax.broadcasted_iota(jnp.int32, (ROWS, 1), 0)
            allowed = kpos <= qpos
        for h in range(2):
            kcat = jnp.concatenate([k[:, h * NOPE : (h + 1) * NOPE], rope], axis=1)
            s = lax.dot_general(
                q_ref[h], kcat, (((1,), (1,)), ((), ())), preferred_element_type=jnp.float32
            )
            s = s * scale
            if masked:
                s = jnp.where(allowed, s, -1e30)
            m_old = m_ref[h]
            m_new = jnp.maximum(m_old, jnp.max(s, axis=1, keepdims=True))
            p = jnp.exp2(s - m_new[:, :1])
            if masked:
                p = jnp.where(allowed, p, 0.0)
            alpha = jnp.exp2(m_old - m_new)
            l_ref[h] = l_ref[h] * alpha + jnp.sum(p, axis=1, keepdims=True)
            acc_ref[h] = acc_ref[h] * alpha + jnp.dot(
                p.astype(jnp.bfloat16),
                v[:, h * VDIM : (h + 1) * VDIM],
                preferred_element_type=jnp.float32,
            )
            m_ref[h] = m_new

    mine = z * NX + x

    def round_(s, carry):
        for k in range(13):

            @pl.when(s == k)
            def _():
                if k < 8:
                    ev_z(k)
                if k == 0:
                    prepare()
                if 0 <= k - 1 < 8:
                    ev_x1(k - 1)
                if 0 <= k - 2 < 8:
                    ev_x2(k - 2)
                if 0 <= k - 3 < 8:
                    ev_y(k - 3, -1)
                    ev_y(k - 3, 1)
                if 0 <= k - 4 < 8:
                    ev_y(k - 4, 2)
                if k == 1:
                    for copy in own_proj:
                        copy.wait()
                if 0 <= k - 1 < 8:
                    ev_proj(k - 1)
                if 0 <= k - 3 < 8:
                    ev_proj1(k - 3)
                if 0 <= k - 5 < 8:
                    ev_proj2(k - 5)

        def pair(d, carry):
            i = s - 1 - jnp.where(d == 0, 0, jnp.where(d == 3, 4, 3))

            @pl.when((i >= 0) & (i < 8))
            def _():
                off = jnp.where(lax.rem(i, 2) == 1, -((i + 1) // 2), i // 2)
                dx = jnp.where(d == 3, 2, jnp.where(d == 1, -1, jnp.where(d == 2, 1, 0)))
                zz = ring(z + off, NZ)
                xx = ring(x + dx, NX)
                for h in range(2):
                    arrived(1 - c, zz, xx, h)
                theirs = zz * NX + xx

                @pl.when(theirs < mine)
                def _():
                    compute(zz, xx, False)

                @pl.when(theirs == mine)
                def _():
                    compute(zz, xx, True)

            return carry

        return lax.fori_loop(0, 4, pair, carry)

    lax.fori_loop(0, 13, round_, 0)

    for h in range(2):
        heads = (acc_ref[h] / l_ref[h]).astype(jnp.bfloat16)
        for q in range(NY):
            HS[q, :, h * VDIM : (h + 1) * VDIM] = heads[q * 64 : (q + 1) * 64]

    def heads_to(yy):
        return pltpu.make_async_remote_copy(
            src_ref=HS.at[yy], dst_ref=HX.at[y], send_sem=hsend.at[yy], recv_sem=hrecv.at[y],
            device_id={"y": yy}, device_id_type=MESH_ID,
        )

    for yy in (y2, ya, yb):
        heads_to(yy).start()
    HX[y] = HS[y]
    for yy in (yb, ya, y2):
        for r in range(8):
            proj_in(yy, 1 - c, r)
    for yy in (yb, ya, y2):
        pltpu.make_async_remote_copy(
            src_ref=HS.at[yy], dst_ref=HX.at[yy], send_sem=hsend.at[yy], recv_sem=hrecv.at[yy],
            device_id={"y": yy}, device_id_type=MESH_ID,
        ).wait_recv()
    squares = jnp.zeros((64, 1), jnp.float32)
    for half in range(2):
        lanes = slice(half * 1024, (half + 1) * 1024)
        total = jnp.zeros((64, 1024), jnp.float32)
        for q in range(NY):
            weight = jnp.concatenate([W[q, half, r] for r in range(8)], axis=0)
            rows = jnp.dot(HX[q], weight, preferred_element_type=jnp.float32)
            total = total + rows.astype(jnp.bfloat16).astype(jnp.float32)
        one = (res_ref[:, lanes].astype(jnp.float32) + total).astype(jnp.bfloat16)
        HID[:, lanes] = one
        one = one.astype(jnp.float32)
        squares = squares + jnp.sum(one * one, axis=1, keepdims=True)
    factor = lax.rsqrt(squares * (1.0 / 2048) + norm_eps)
    gain = fg_ref[...].astype(jnp.float32).reshape(1, 2048)
    for b in range(SUBS):
        lanes = slice(b * WIDE, (b + 1) * WIDE)
        COL[0, b] = (
            HID[:, lanes].astype(jnp.float32) * factor * gain[:, lanes]
        ).astype(jnp.bfloat16)
    experts_part(
        z, x, c, y, up, down, peers, weights, out_ref,
        T, HID, ACC, COL, OUT, ARR, EO, RET, PART, RD, RU, wg, wu, wd, sg, su, sd,
        ezrecv, ezsend, arecv, asend, rrecv, rsend, drecv, dsend, elsem,
    )
    for yy in (y2, ya, yb):
        heads_to(yy).wait_send()
    pltpu.make_async_remote_copy(
        src_ref=W.at[0:3, 0], dst_ref=W.at[0:3, 0], send_sem=wcsend, recv_sem=wrecv.at[0, 0, 0],
        device_id=mate, device_id_type=MESH_ID,
    ).wait_send()
    for wait in sent:
        wait()
    whole = G.at[c]
    pltpu.make_async_remote_copy(
        src_ref=whole, dst_ref=whole, send_sem=csend, recv_sem=recv.at[0, 0, 0, 0],
        device_id=mate, device_id_type=MESH_ID,
    ).wait_send()


def layer(small, large):
    vmem = pl.BlockSpec(memory_space=pltpu.VMEM)
    hbm = pl.BlockSpec(memory_space=pl.ANY)
    bf, f32, dma = jnp.bfloat16, jnp.float32, pltpu.SemaphoreType.DMA
    d, f = large[3].shape
    shapes = [
        ((2, NZ, NX, 2, HALF, 256), bf),
        ((NZ, 8, 128), f32),
        ((2, ROWS, 128), f32),
        ((2, ROWS, 128), f32),
        ((2, ROWS, 128), f32),
        ((NY, 2, 8, 32, 1024), bf),
        ((NY, 64, 256), bf),
        ((NY, 64, 256), bf),
        ((2, ROWS, 256), bf),
        ((256, 256), bf),
        ((256, 256), bf),
        ((64, d), bf),
        ((64, d), f32),
        ((8, SUBS, 64, WIDE), bf),
        ((8, 8, CAP, d), bf),
        ((8, 8, CAP, d), bf),
        ((8, 8, CAP, d), bf),
        ((8, 8, CAP, d), bf),
        ((8, SUBS, 64, WIDE), bf),
        ((4, SUBS, 64, WIDE), bf),
        ((4, SUBS, 64, WIDE), bf),
        ((d, f), bf),
        ((d, f), bf),
        ((f, d), bf),
        ((d, f), bf),
        ((d, f), bf),
        ((f, d), bf),
    ]
    sems = [
        (2, NZ, NX, 2), (NZ,), (2, 4, 2), (2, 4), (8, 2), (8,), (8, 3), (), (4,),
        (NY, 2, 8), (2, 8), (8,), (), (NY,), (NY,), (2,), (6,),
        (8, SUBS), (8, SUBS), (8,), (8,), (8,), (8,), (2, 4, SUBS), (2, 4, SUBS), (3,),
    ]
    return pl.pallas_call(
        gather_attend_kernel,
        out_shape=jax.ShapeDtypeStruct((64, 2048), jnp.bfloat16),
        in_specs=[vmem] * len(small) + [hbm] * len(large),
        out_specs=vmem,
        scratch_shapes=[pltpu.VMEM(*shape) for shape in shapes]
        + [dma(shape) if shape else dma for shape in sems],
        compiler_params=pltpu.CompilerParams(
            collective_id=0, has_side_effects=True, vmem_limit_bytes=63 * 1024 * 1024
        ),
    )(*small, *large)


def experts_part(
    z, x, c, y, up, down, peers, weights, out_ref,
    T, HID, ACC, COL, OUT, ARR, EO, RET, PART, RD, RU, wg, wu, wd, sg, su, sd,
    zrecv, zsend, arecv, asend, rrecv, rsend, drecv, dsend, lsem,
):
    me = x * NC + c

    at = {off: i for i, off in enumerate(OFFS)}

    def along_z(i, b, dev, off_to, n):
        there = at[off_to]
        return pltpu.make_async_remote_copy(
            src_ref=COL.at[i, b], dst_ref=COL.at[there, b], send_sem=zsend.at[n, b],
            recv_sem=zrecv.at[there, b], device_id=dev, device_id_type=MESH_ID,
        )

    def pass_on(off, b):
        i = at[off]
        if off != 0:
            along_z(i, b, up, off, 0).wait_recv()
        if -3 < off <= 0 or (off == -3 and b < 2):
            start(along_z(i, b, up, off - 1, -off))
        if 0 <= off < 3:
            start(along_z(i, b, down, off + 1, 4 + off))
        if off == 3 and b >= 2:
            start(along_z(i, b, down, -4, 7))

    sends = []

    def start(copy):
        copy.start()
        sends.append(copy)

    def pieces(i, src, dst, sems_send, sems_recv):
        for p, dev in peers:
            pltpu.make_async_remote_copy(
                src_ref=src.at[i, p], dst_ref=dst.at[i, me], send_sem=sems_send.at[i],
                recv_sem=sems_recv.at[i], device_id=dev, device_id_type=MESH_ID,
            ).start()
        pltpu.make_async_copy(src.at[i, me], dst.at[i, me], lsem.at[1]).start()
        pltpu.make_async_copy(src.at[i, me], dst.at[i, me], lsem.at[1]).wait()

    def pieces_in(i, dst, sems_recv):
        ref = dst.at[i, 0:7]
        pltpu.make_async_remote_copy(
            src_ref=ref, dst_ref=ref, send_sem=lsem.at[2], recv_sem=sems_recv.at[i],
            device_id=peers[0][1], device_id_type=MESH_ID,
        ).wait_recv()

    def pieces_sent(i, src, sems_send):
        ref = src.at[i, 0:7]
        pltpu.make_async_remote_copy(
            src_ref=ref, dst_ref=ref, send_sem=sems_send.at[i], recv_sem=lsem.at[2],
            device_id=peers[0][1], device_id_type=MESH_ID,
        ).wait_send()

    slots = lax.broadcasted_iota(jnp.int32, (64, 64), 0).astype(jnp.float32)

    def matches(i):
        tab = T[ring(z + OFFS[i], NZ)]
        base = (z * 64).astype(jnp.float32)
        return [(tab[k : k + 1, 0:64] - base) == slots for k in range(4)], tab

    def picks(i):
        hit, _ = matches(i)
        return jnp.where(hit[0] | hit[1] | hit[2] | hit[3], 1.0, 0.0).astype(jnp.bfloat16)

    def select(i, b, pick):
        rows = jnp.dot(pick, COL[i, b], preferred_element_type=jnp.float32)
        for p in range(8):
            OUT[i, p, :, b * WIDE : (b + 1) * WIDE] = rows[p * CAP : (p + 1) * CAP].astype(
                jnp.bfloat16
            )

    def gated(rows, gate, upper, lower):
        g = jnp.dot(rows, gate[...], preferred_element_type=jnp.float32)
        u = jnp.dot(rows, upper[...], preferred_element_type=jnp.float32)
        hidden = (g / (1.0 + jnp.exp(-g)) * u).astype(jnp.bfloat16)
        return jnp.dot(hidden, lower[...], preferred_element_type=jnp.float32)

    def expert(group):
        for i in group:
            pieces_in(i, ARR, arecv)
        rows = jnp.concatenate(
            [ARR[i, p].astype(jnp.float32) for i in group for p in range(8)], axis=0
        ).astype(jnp.bfloat16)
        done = gated(rows, wg, wu, wd)
        for n, i in enumerate(group):
            for p in range(8):
                lo = (n * 8 + p) * CAP
                EO[i, p] = done[lo : lo + CAP].astype(jnp.bfloat16)

    def combine(i):
        pieces_in(i, RET, rrecv)
        hit, tab = matches(i)
        share = jnp.zeros((64, 64), jnp.float32)
        for k in range(4):
            share = share + jnp.where(hit[k], tab[4 + k : 5 + k, 0:64], 0.0)
        hi = share.astype(jnp.bfloat16)
        lo = (share - hi.astype(jnp.float32)).astype(jnp.bfloat16)
        back = jnp.concatenate(
            [RET[i, p].astype(jnp.float32) for p in range(8)], axis=0
        ).astype(jnp.bfloat16)
        dims = (((0,), (0,)), ((), ()))
        total = lax.dot_general(hi, back, dims, preferred_element_type=jnp.float32)
        total = total + lax.dot_general(lo, back, dims, preferred_element_type=jnp.float32)
        for b in range(SUBS):
            PART[i, b] = total[:, b * WIDE : (b + 1) * WIDE].astype(jnp.bfloat16)

    groups = ((0,), (1, 2), (3, 4), (5, 6), (7,))

    def shared():
        for w in weights[3:]:
            w.wait()
        rows = jnp.concatenate([COL[0, b] for b in range(SUBS)], axis=1)
        ACC[...] = (
            HID[...].astype(jnp.float32)
            + gated(rows, sg, su, sd).astype(jnp.bfloat16).astype(jnp.float32)
        )

    def between(s, b):
        if s >= 2 and b == 1:
            if s == 2:
                for w in weights[:3]:
                    w.wait()
            expert(groups[s - 2])

    for s in range(5):
        pick = [picks(i) for i in groups[s]]
        for b in range(SUBS):
            for n, i in enumerate(groups[s]):
                pass_on(OFFS[i], b)
            for n, i in enumerate(groups[s]):
                select(i, b, pick[n])
            between(s, b)
        for i in groups[s]:
            pieces(i, OUT, ARR, asend, arecv)
    expert(groups[3])
    expert(groups[4])
    for group in reversed(groups):
        for i in group:
            pieces(i, EO, RET, rsend, rrecv)
    shared()

    def back_z(i, b, way, k):
        dst, dev = ((RD, down), (RU, up))[way]
        return pltpu.make_async_remote_copy(
            src_ref=PART.at[i, b], dst_ref=dst.at[k, b], send_sem=dsend.at[way, k, b],
            recv_sem=drecv.at[way, k, b], device_id=dev, device_id_type=MESH_ID,
        )

    def chain(way, k, b):
        i = at[-k if way == 0 or k == 4 else k]
        if k < 3 or (k == 3 and (b < 2) == (way == 0)):
            back_z(i, b, way, k).wait_recv()
            dst = (RD, RU)[way]
            PART[i, b] = (
                PART[i, b].astype(jnp.float32) + dst[k, b].astype(jnp.float32)
            ).astype(jnp.bfloat16)
        start(back_z(i, b, way, k - 1))

    combine(7)
    for n in range(2):
        chain(0, 4, n)
        chain(1, 4, n + 2)
    for k in (3, 2, 1):
        for i in groups[k]:
            combine(i)
        for n in range(4):
            chain(0, k, (n + 2) % 4)
            chain(1, k, n)
    combine(0)
    for n in range(4):
        back_z(0, n, 0, 0).wait_recv()
        back_z(0, n, 1, 0).wait_recv()
        lanes = slice(n * WIDE, (n + 1) * WIDE)
        routed = (
            PART[0, n].astype(jnp.float32)
            + RD[0, n].astype(jnp.float32)
            + RU[0, n].astype(jnp.float32)
        )
        total = ACC[:, lanes] + routed.astype(jnp.bfloat16).astype(jnp.float32)
        out_ref[:, lanes] = total.astype(jnp.bfloat16)

    for copy in sends:
        copy.wait_send()
    for i in range(8):
        pieces_sent(i, OUT, asend)
        pieces_sent(i, EO, rsend)


def body(
    query_nope,
    query_rope,
    latent,
    key_rope,
    latent_gain,
    key_up,
    value_up,
    out_proj,
    residual,
    ffn_gain,
    expert_ids,
    route_weights,
    expert_gate,
    expert_up,
    expert_down,
    shared_gate,
    shared_up,
    shared_down,
):
    z, x, core, y = (lax.axis_index(n) for n in ("z", "x", "core", "y"))
    q_sp = (z * NX + x) * NC + core
    first_row = q_sp * ROWS
    positions = first_row + jnp.arange(ROWS, dtype=jnp.int32)
    half_dim = ROPE // 2
    frequency = rope_base ** (-jnp.arange(half_dim, dtype=jnp.float32) / half_dim)
    angles = positions.astype(jnp.float32)[:, None] * jnp.concatenate([frequency] * 4)[None, :]
    sign = jnp.where(jnp.arange(128) % ROPE < half_dim, -1.0, 1.0)
    cosine, sine_part = jnp.cos(angles), jnp.sin(angles) * sign[None, :]

    small = (
        latent, key_rope.T, query_nope, query_rope, cosine, sine_part, latent_gain,
        expert_ids.T, route_weights.T, residual, ffn_gain,
    )
    large = (
        key_up, value_up, out_proj.reshape(8, 32, 2048), expert_gate[0], expert_up[0],
        expert_down[0], shared_gate, shared_up, shared_down,
    )
    return layer(small, large)


def solution(mesh):
    fine = Mesh(mesh.devices.reshape(NZ, NX, NC, NY), ("z", "x", "core", "y"))
    sp = ("z", "x", "core")
    every = ("z", "x", "core", "y")
    in_specs = (
        P(sp, "y"),
        P(sp, "y"),
        P(sp, None),
        P(sp, None),
        P(),
        P(),
        P(),
        P("y", None),
        P(every, None),
        P(),
        P(every, None),
        P(every, None),
        P(sp, None, None),
        P(sp, None, None),
        P(sp, None, None),
        P(),
        P(),
        P(),
    )
    return jax.shard_map(
        body, mesh=fine, in_specs=in_specs, out_specs=P(every, None), check_vma=False
    )
```
